32 devices in a mesh: sp: 4 (over z), dp: 8 (over y, x, core).
Axes of the slice: x: 2, y: 2, z: 4, core: 2. Of those that a mesh axis runs over, the one named last changes fastest.
Arguments:
- inputs: bfloat16 [8, 512, 2048], P('dp', 'sp'), may hold values from -0.75 to 0.75
- queries: bfloat16 [8, 512, 1024], P('dp', 'sp'), may hold values from -18 to 18
- keys: bfloat16 [8, 512, 256], P('dp', 'sp'), may hold values from -18 to 18
- values: bfloat16 [8, 512, 256], P('dp', 'sp'), may hold values from -6 to 6
- out_grad: bfloat16 [8, 512, 1024], P('dp', 'sp'), may hold values from -144 to 144
- query_gain: float32 [64], replicated, may hold values from 0.4 to 6.5
- key_gain: float32 [64], replicated, may hold values from 0.4 to 6.5
- key_matrix: bfloat16 [2048, 256], P('dp'), may hold values from -0.125 to 0.125
- value_matrix: bfloat16 [2048, 256], P('dp'), may hold values from -0.125 to 0.125
Outputs:
- input_grad: bfloat16 [8, 512, 2048], P('dp', 'sp')
- query_grad: bfloat16 [8, 512, 1024], P('dp', 'sp')
- key_weight_grad: float32 [2048, 256], P('dp')
- value_weight_grad: float32 [2048, 256], P('dp')
The draws below stay inside these ranges and needn't reach their ends.
All inputs are finite; a program needn't handle non-finite values.
Results may differ from the reference program's by a relative error of at most 0.024.
The reference program's roundings to bfloat16 on the way count: a program that leaves them out, or rounds other values in their place, can miss the bound.
Values may be sent and summed in bfloat16 or wider, within the bound.
No kernel may reach another device: no remote copies, remote signals or barrier semaphores. Data moves between devices by JAX's collectives and lax.ppermute only.
A program may use at most 64 MiB of HBM per device.

```python
import jax
import jax.numpy as jnp
from jax import lax

MODEL_WIDTH = 2048
QUERY_HEADS = 16
KEY_VALUE_HEADS = 4
HEAD_CHANNELS = 64
GRID = 64
SEQUENCE_LENGTH = 512
SEQUENCE_COUNT = 8
HPART = 4


def gain_draw(seed_key):
    return jnp.clip(1.0 + 0.18 * jax.random.normal(seed_key, (HEAD_CHANNELS,), jnp.float32), 0.4, 1.6)


def draw_query_gain(key, part):
    return gain_draw(jax.random.fold_in(key, 11))


def draw_key_gain(key, part):
    return gain_draw(jax.random.fold_in(key, 23))


def level_of(stream_key, extent, cuts, low, largest):
    def one(dim, parts):
        steps = jax.random.uniform(jax.random.fold_in(jax.random.fold_in(stream_key, 6), dim), (parts,), jnp.float32, low / len(cuts), largest / len(cuts))
        return jnp.repeat(jnp.exp(steps), extent[dim] // parts).reshape((-1,) + (1,) * (len(extent) - dim - 1))

    level = one(*cuts[0])
    for cut in cuts[1:]:
        level = level * one(*cut)
    return level


def bell_draw(rng, shape, deviation, limit, shards=(), kind=jnp.bfloat16):
    entries = jax.random.normal(rng, shape, jnp.float32) * deviation
    if len(shards) > 0:
        entries = level_of(rng, shape, shards, -0.22, 0.18) * entries
    return jnp.clip(entries, min=-limit, max=limit).astype(kind)


def setup_inputs(seed: int = 0) -> dict:
    arg_keys = jax.random.split(jax.random.key(seed), 10)
    return {
        "inputs": bell_draw(arg_keys[0], (SEQUENCE_COUNT, SEQUENCE_LENGTH, MODEL_WIDTH), 0.125, 0.75, ((0, 8), (1, 4))),
        "queries": bell_draw(arg_keys[1], (SEQUENCE_COUNT, SEQUENCE_LENGTH, QUERY_HEADS * HEAD_CHANNELS), 3.0, 18.0, ((0, 8), (1, 4))),
        "keys": bell_draw(arg_keys[2], (SEQUENCE_COUNT, SEQUENCE_LENGTH, KEY_VALUE_HEADS * HEAD_CHANNELS), 3.0, 18.0, ((0, 8), (1, 4))),
        "values": bell_draw(arg_keys[3], (SEQUENCE_COUNT, SEQUENCE_LENGTH, KEY_VALUE_HEADS * HEAD_CHANNELS), 1.0, 6.0, ((0, 8), (1, 4))),
        "out_grad": bell_draw(arg_keys[4], (SEQUENCE_COUNT, SEQUENCE_LENGTH, QUERY_HEADS * HEAD_CHANNELS), 24.0, 144.0, ((0, 8), (1, 4))),
        "query_gain": draw_query_gain(jax.random.fold_in(arg_keys[9], 71), 0),
        "key_gain": draw_key_gain(jax.random.fold_in(arg_keys[9], 71), 0),
        "key_matrix": bell_draw(arg_keys[7], (MODEL_WIDTH, KEY_VALUE_HEADS * HEAD_CHANNELS), MODEL_WIDTH ** -0.5, 0.125, ((0, 8),)),
        "value_matrix": bell_draw(arg_keys[8], (MODEL_WIDTH, KEY_VALUE_HEADS * HEAD_CHANNELS), MODEL_WIDTH ** -0.5, 0.125, ((0, 8),)),
    }


rope_base = 10000.0
norm_eps = 0.5
score_scale = 0.125

def product(pattern, first_op, second_op):
    return jnp.einsum(pattern, first_op.astype(jnp.float32), second_op.astype(jnp.float32))

def rotary_tables(token_length):
    position = jnp.arange(token_length, dtype=jnp.int32)
    grid_row = (position // GRID).astype(jnp.float32)
    grid_col = (position % GRID).astype(jnp.float32)
    half_pairs = HEAD_CHANNELS // 4
    inv_freq = rope_base ** (-jnp.arange(half_pairs, dtype=jnp.float32) / half_pairs)
    angles = jnp.concatenate([grid_row[:, None] * inv_freq, grid_col[:, None] * inv_freq], axis=1)
    return (jnp.cos(angles), jnp.sin(angles))

def rotate(vector, cos_tab, sin_tab):
    even_part = vector[..., 0::2]
    odd_part = vector[..., 1::2]
    turned = jnp.stack([even_part * cos_tab - odd_part * sin_tab, even_part * sin_tab + odd_part * cos_tab], axis=-1)
    return turned.reshape(vector.shape)

def rotate_back(cotangent, cos_tab, sin_tab):
    even_part = cotangent[..., 0::2]
    odd_part = cotangent[..., 1::2]
    turned = jnp.stack([even_part * cos_tab + odd_part * sin_tab, odd_part * cos_tab - even_part * sin_tab], axis=-1)
    return turned.reshape(cotangent.shape)

def inverse_rms(vector):
    return lax.rsqrt(lax.optimization_barrier(jnp.mean(vector * vector, axis=-1, keepdims=True)) + norm_eps)

def norm_back(vector, inv_scale, cotangent, gain_vec):
    weighted = cotangent * gain_vec
    inner_mean = lax.optimization_barrier(jnp.mean(weighted * vector, axis=-1, keepdims=True))
    return inv_scale * (weighted - vector * inv_scale * inv_scale * inner_mean)

def head_grads(query_in, key_input, value_input, grad_in, query_gain, key_gain, cos_tab, sin_tab, block_rows):
    token_length, groups, per_group, head_dim = query_in.shape
    cos_four = cos_tab[:, None, None, :]
    sin_four = sin_tab[:, None, None, :]
    cos_three = cos_tab[:, None, :]
    sin_three = sin_tab[:, None, :]
    query_f = query_in.astype(jnp.float32)
    query_inv = inverse_rms(query_f)
    query_rot = rotate(query_f * query_inv * query_gain, cos_four, sin_four).astype(jnp.bfloat16)
    key_f = key_input.astype(jnp.float32)
    key_inv = inverse_rms(key_f)
    key_rot = rotate(key_f * key_inv * key_gain, cos_three, sin_three).astype(jnp.bfloat16)
    num_blocks = token_length // block_rows
    query_blocks = query_rot.reshape(num_blocks, block_rows, groups, per_group, head_dim)
    grad_blocks = grad_in.reshape(num_blocks, block_rows, groups, per_group, head_dim)

    def attend_block(carried, pieces):
        key_acc, value_acc = carried
        query_piece, grad_piece = pieces
        scores = product('qgrd,cgd->grqc', query_piece, key_rot) * score_scale
        row_max = lax.optimization_barrier(jnp.max(scores, axis=-1, keepdims=True))
        shifted = jnp.exp(scores - row_max)
        attn_prob = shifted / lax.optimization_barrier(jnp.sum(shifted, axis=-1, keepdims=True))
        prob_low = attn_prob.astype(jnp.bfloat16)
        prob_grad = product('qgrd,cgd->grqc', grad_piece, value_input)
        row_dot = lax.optimization_barrier(jnp.sum(attn_prob * prob_grad, axis=-1, keepdims=True))
        score_grad = (attn_prob * (prob_grad - row_dot) * score_scale).astype(jnp.bfloat16)
        dq_piece = product('grqc,cgd->qgrd', score_grad, key_rot)
        key_acc = key_acc + product('grqc,qgrd->cgd', score_grad, query_piece)
        value_acc = value_acc + product('grqc,qgrd->cgd', prob_low, grad_piece)
        return ((key_acc, value_acc), dq_piece)
    empty_acc = jnp.zeros((token_length, groups, head_dim), jnp.float32)
    (key_rot_grad, value_acc), query_rot_grad = lax.scan(attend_block, (empty_acc, empty_acc), (query_blocks, grad_blocks))
    query_rot_grad = query_rot_grad.reshape(token_length, groups, per_group, head_dim)
    query_grad = norm_back(query_f, query_inv, rotate_back(query_rot_grad, cos_four, sin_four), query_gain).astype(jnp.bfloat16)
    key_portion = norm_back(key_f, key_inv, rotate_back(key_rot_grad, cos_three, sin_three), key_gain).astype(jnp.bfloat16)
    return (query_grad, key_portion, value_acc.astype(jnp.bfloat16))

def reference(inputs, queries, keys, values, out_grad, query_gain, key_gain, key_matrix, value_matrix):
    token_length = queries.shape[1]
    portion_count = QUERY_HEADS // HPART
    group_copies = portion_count // KEY_VALUE_HEADS
    cos_tab, sin_tab = rotary_tables(token_length)
    block_rows = min(512, token_length)

    def sequence_grads(pack):
        query_in, key_input, value_input, grad_in = pack
        key_positions = jnp.repeat(key_input.reshape(token_length, KEY_VALUE_HEADS, HEAD_CHANNELS), group_copies, axis=1)
        value_positions = jnp.repeat(value_input.reshape(token_length, KEY_VALUE_HEADS, HEAD_CHANNELS), group_copies, axis=1)
        query_part, key_portion, value_portion = head_grads(query_in.reshape(token_length, portion_count, HPART, HEAD_CHANNELS), key_positions, value_positions, grad_in.reshape(token_length, portion_count, HPART, HEAD_CHANNELS), query_gain, key_gain, cos_tab, sin_tab, block_rows)
        key_gradient = key_portion.reshape(token_length, KEY_VALUE_HEADS, group_copies, HEAD_CHANNELS).astype(jnp.float32).sum(axis=2).astype(jnp.bfloat16)
        value_gradient = value_portion.reshape(token_length, KEY_VALUE_HEADS, group_copies, HEAD_CHANNELS).astype(jnp.float32).sum(axis=2).astype(jnp.bfloat16)
        joined_output = jnp.concatenate([key_gradient.reshape(token_length, KEY_VALUE_HEADS * HEAD_CHANNELS), value_gradient.reshape(token_length, KEY_VALUE_HEADS * HEAD_CHANNELS)], axis=1)
        return (query_part.reshape(token_length, QUERY_HEADS * HEAD_CHANNELS), joined_output)
    query_grad, projection_gradient = lax.map(sequence_grads, (queries, keys, values, out_grad))
    joined_weight = jnp.concatenate([key_matrix, value_matrix], axis=1)
    flattened_gradient = projection_gradient.reshape(-1, 2 * KEY_VALUE_HEADS * HEAD_CHANNELS)
    input_grad = jnp.dot(flattened_gradient, joined_weight.T, preferred_element_type=jnp.float32).astype(jnp.bfloat16)
    input_grad = input_grad.reshape(inputs.shape)
    weight_grad = jnp.dot(inputs.reshape(-1, inputs.shape[2]).T, flattened_gradient, preferred_element_type=jnp.float32)
    key_value_width = KEY_VALUE_HEADS * HEAD_CHANNELS
    return (input_grad, query_grad, weight_grad[:, :key_value_width], weight_grad[:, key_value_width:])
```

```python
import jax
import jax.numpy as jnp
import numpy as np
from jax import lax
from jax.experimental import pallas as pl
from jax.experimental.pallas import tpu as pltpu
from jax.sharding import PartitionSpec as P

QUERY_HEADS = 16
KEY_VALUE_HEADS = 4
HEAD_CHANNELS = 64
GRID = 64


rope_base = 10000.0
norm_eps = 0.5
score_scale = 0.125


def product(pattern, first_op, second_op):
    return jnp.einsum(pattern, first_op, second_op, preferred_element_type=jnp.float32)


def rotary_tables(token_length):
    position = jnp.arange(token_length, dtype=jnp.int32)
    grid_row = (position // GRID).astype(jnp.float32)
    grid_col = (position % GRID).astype(jnp.float32)
    half_pairs = HEAD_CHANNELS // 4
    inv_freq = rope_base ** (-jnp.arange(half_pairs, dtype=jnp.float32) / half_pairs)
    angles = jnp.concatenate([grid_row[:, None] * inv_freq, grid_col[:, None] * inv_freq], axis=1)
    return (jnp.cos(angles), jnp.sin(angles))


def rotate(vector, cos_tab, sin_tab):
    even_part = vector[..., 0::2]
    odd_part = vector[..., 1::2]
    turned = jnp.stack(
        [even_part * cos_tab - odd_part * sin_tab, even_part * sin_tab + odd_part * cos_tab],
        axis=-1,
    )
    return turned.reshape(vector.shape)


def rotate_back(cotangent, cos_tab, sin_tab):
    even_part = cotangent[..., 0::2]
    odd_part = cotangent[..., 1::2]
    turned = jnp.stack(
        [even_part * cos_tab + odd_part * sin_tab, odd_part * cos_tab - even_part * sin_tab],
        axis=-1,
    )
    return turned.reshape(cotangent.shape)


def inverse_rms(vector):
    return lax.rsqrt(jnp.mean(vector * vector, axis=-1, keepdims=True) + norm_eps)


def norm_back(vector, inv_scale, cotangent, gain_vec):
    weighted = cotangent * gain_vec
    inner_mean = jnp.mean(weighted * vector, axis=-1, keepdims=True)
    return inv_scale * (weighted - vector * inv_scale * inv_scale * inner_mean)


def head_grads(
    query_in, key_input, value_input, grad_in, query_gain, key_gain, cos_tab, sin_tab, block_rows
):
    token_length, groups, per_group, head_dim = query_in.shape
    cos_four = cos_tab[:, None, None, :]
    sin_four = sin_tab[:, None, None, :]
    cos_three = cos_tab[:, None, :]
    sin_three = sin_tab[:, None, :]
    query_f = query_in.astype(jnp.float32)
    query_inv = inverse_rms(query_f)
    query_rot = rotate(query_f * query_inv * query_gain, cos_four, sin_four).astype(jnp.bfloat16)
    key_f = key_input.astype(jnp.float32)
    key_inv = inverse_rms(key_f)
    key_rot = rotate(key_f * key_inv * key_gain, cos_three, sin_three).astype(jnp.bfloat16)
    num_blocks = token_length // block_rows
    query_blocks = query_rot.reshape(num_blocks, block_rows, groups, per_group, head_dim)
    grad_blocks = grad_in.reshape(num_blocks, block_rows, groups, per_group, head_dim)

    def attend_block(carried, pieces):
        key_acc, value_acc = carried
        query_piece, grad_piece = pieces
        scores = product("qgrd,cgd->grqc", query_piece, key_rot) * score_scale
        row_max = jnp.max(scores, axis=-1, keepdims=True)
        shifted = jnp.exp(scores - row_max)
        attn_prob = shifted / jnp.sum(shifted, axis=-1, keepdims=True)
        prob_low = attn_prob.astype(jnp.bfloat16)
        prob_grad = product("qgrd,cgd->grqc", grad_piece, value_input)
        row_dot = jnp.sum(attn_prob * prob_grad, axis=-1, keepdims=True)
        score_grad = (attn_prob * (prob_grad - row_dot) * score_scale).astype(jnp.bfloat16)
        dq_piece = product("grqc,cgd->qgrd", score_grad, key_rot)
        key_acc = key_acc + product("grqc,qgrd->cgd", score_grad, query_piece)
        value_acc = value_acc + product("grqc,qgrd->cgd", prob_low, grad_piece)
        return ((key_acc, value_acc), dq_piece)

    empty_acc = jnp.zeros((token_length, groups, head_dim), jnp.float32)
    (key_rot_grad, value_acc), query_rot_grad = lax.scan(
        attend_block, (empty_acc, empty_acc), (query_blocks, grad_blocks)
    )
    query_rot_grad = query_rot_grad.reshape(token_length, groups, per_group, head_dim)
    query_grad = norm_back(
        query_f, query_inv, rotate_back(query_rot_grad, cos_four, sin_four), query_gain
    ).astype(jnp.bfloat16)
    key_portion = norm_back(
        key_f, key_inv, rotate_back(key_rot_grad, cos_three, sin_three), key_gain
    ).astype(jnp.bfloat16)
    return (query_grad, key_portion, value_acc.astype(jnp.bfloat16))


def generic_device(
    inputs, queries, keys, values, out_grad, query_gain, key_gain, key_matrix, value_matrix
):
    sp_count = lax.axis_size("sp")
    dp_count = lax.axis_size("dp")
    token_row_block = inputs.shape[1]
    token_length = token_row_block * sp_count
    local_heads = QUERY_HEADS // sp_count
    portion_heads = min(local_heads, QUERY_HEADS // KEY_VALUE_HEADS)
    kv_here = local_heads // portion_heads
    group_copies = QUERY_HEADS // KEY_VALUE_HEADS // portion_heads
    key_value_width = KEY_VALUE_HEADS * HEAD_CHANNELS
    key_positions = jnp.repeat(
        keys[0].reshape(token_row_block, KEY_VALUE_HEADS, HEAD_CHANNELS), group_copies, axis=1
    ).reshape(token_row_block, key_value_width * group_copies)
    value_positions = jnp.repeat(
        values[0].reshape(token_row_block, KEY_VALUE_HEADS, HEAD_CHANNELS), group_copies, axis=1
    ).reshape(token_row_block, key_value_width * group_copies)
    grad_heads, query_heads, key_heads, value_heads = (
        lax.all_to_all(out_grad[0], "sp", split_axis=1, concat_axis=0, tiled=True),
        lax.all_to_all(queries[0], "sp", split_axis=1, concat_axis=0, tiled=True),
        lax.all_to_all(key_positions, "sp", split_axis=1, concat_axis=0, tiled=True),
        lax.all_to_all(value_positions, "sp", split_axis=1, concat_axis=0, tiled=True),
    )
    cos_tab, sin_tab = rotary_tables(token_length)
    query_part, key_portion, value_portion = head_grads(
        query_heads.reshape(token_length, kv_here, portion_heads, HEAD_CHANNELS),
        key_heads.reshape(token_length, kv_here, HEAD_CHANNELS),
        value_heads.reshape(token_length, kv_here, HEAD_CHANNELS),
        grad_heads.reshape(token_length, kv_here, portion_heads, HEAD_CHANNELS),
        query_gain,
        key_gain,
        cos_tab,
        sin_tab,
        min(512, token_length),
    )
    query_tokens, key_token_rows, value_token_rows = (
        lax.all_to_all(
            query_part.reshape(token_length, local_heads * HEAD_CHANNELS),
            "sp",
            split_axis=0,
            concat_axis=1,
            tiled=True,
        ),
        lax.all_to_all(
            key_portion.reshape(token_length, kv_here * HEAD_CHANNELS),
            "sp",
            split_axis=0,
            concat_axis=1,
            tiled=True,
        ),
        lax.all_to_all(
            value_portion.reshape(token_length, kv_here * HEAD_CHANNELS),
            "sp",
            split_axis=0,
            concat_axis=1,
            tiled=True,
        ),
    )
    key_gradient = (
        key_token_rows.reshape(token_row_block, KEY_VALUE_HEADS, group_copies, HEAD_CHANNELS)
        .astype(jnp.float32)
        .sum(axis=2)
        .astype(jnp.bfloat16)
    )
    value_gradient = (
        value_token_rows.reshape(token_row_block, KEY_VALUE_HEADS, group_copies, HEAD_CHANNELS)
        .astype(jnp.float32)
        .sum(axis=2)
        .astype(jnp.bfloat16)
    )
    projection_gradient = jnp.concatenate(
        [
            key_gradient.reshape(token_row_block, key_value_width),
            value_gradient.reshape(token_row_block, key_value_width),
        ],
        axis=1,
    )
    joined_weight = jnp.concatenate([key_matrix, value_matrix], axis=1)
    input_grad = lax.dot_general(
        projection_gradient,
        lax.all_gather(joined_weight, "dp", axis=0, tiled=True),
        (((1,), (1,)), ((), ())),
        preferred_element_type=jnp.float32,
    ).astype(jnp.bfloat16)
    token_in = inputs[0]
    width = inputs.shape[2]
    row_share = width // (sp_count * dp_count)
    permuted = (
        token_in.reshape(token_row_block, dp_count, sp_count, row_share)
        .transpose(0, 2, 1, 3)
        .reshape(token_row_block, width)
    )
    share_cols = lax.all_to_all(permuted, "sp", split_axis=1, concat_axis=0, tiled=True)
    all_grads = lax.all_gather(projection_gradient, "sp", axis=0, tiled=True)
    grad_piece = lax.psum_scatter(
        lax.dot_general(
            share_cols, all_grads, (((0,), (0,)), ((), ())), preferred_element_type=jnp.float32
        ).astype(jnp.bfloat16),
        "dp",
        scatter_dimension=0,
        tiled=True,
    ).astype(jnp.float32)
    weight_grad = lax.all_gather(grad_piece, "sp", axis=0, tiled=True)
    return (
        input_grad[None],
        query_tokens[None],
        weight_grad[:, :key_value_width],
        weight_grad[:, key_value_width:],
    )


bf16 = jnp.bfloat16
f32 = jnp.float32


def dot(first_op, second_op, first_dim, second_dim):
    return lax.dot_general(
        first_op, second_op, (((first_dim,), (second_dim,)), ((), ())), preferred_element_type=f32
    )


def kernel_call(body, out_shape, scratch, args, flops=0, name=None):
    vmem = pl.BlockSpec(memory_space=pltpu.VMEM)
    return pl.pallas_call(
        body,
        out_shape=out_shape,
        in_specs=[vmem] * len(args),
        out_specs=jax.tree.map(lambda _: vmem, out_shape),
        scratch_shapes=scratch,
        cost_estimate=pl.CostEstimate(flops=flops, bytes_accessed=0, transcendentals=0),
        compiler_params=pltpu.CompilerParams(vmem_limit_bytes=60000 * 1024),
        name=name,
    )(*args)


def shape_of(shape, dtype=bf16):
    return jax.ShapeDtypeStruct(shape, dtype)


def exchange(pieces, axis, order):
    count = lax.axis_size(axis)
    received = {0: pieces[0]}
    for k in order:
        received[k] = lax.ppermute(pieces[k], axis, [(i, i ^ k) for i in range(count)])
    return [received[k] for k in range(count)]


def pack_heads(queries, keys, values, out_grad, sp_count):
    rows = queries.shape[0]
    q_width = queries.shape[1] // sp_count
    k_width = keys.shape[1] // sp_count
    width = 2 * q_width + 2 * k_width

    def body(q_ref, g_ref, k_ref, v_ref, *rest):
        outs, buf = rest[:-1], rest[-1]
        me = lax.axis_index("sp")
        for d in range(sp_count):
            buf[d, :, :q_width] = q_ref[:, d * q_width : (d + 1) * q_width]
            buf[d, :, q_width : 2 * q_width] = g_ref[:, d * q_width : (d + 1) * q_width]
            buf[d, :, 2 * q_width :] = jnp.concatenate(
                [
                    k_ref[:, d * k_width : (d + 1) * k_width],
                    v_ref[:, d * k_width : (d + 1) * k_width],
                ],
                axis=1,
            )
        for k, out in enumerate(outs):
            out[...] = buf[me ^ k]

    return kernel_call(
        body,
        [shape_of((rows, width))] * sp_count,
        [pltpu.VMEM((sp_count, rows, width), bf16)],
        (queries, out_grad, keys, values),
        name="pack_heads",
    )


def pack_features(token_in, key_matrix, value_matrix, sp_count, dp_count):
    rows, width = token_in.shape
    share = width // (sp_count * dp_count)
    feats = dp_count * share
    w_rows, kv_width = key_matrix.shape

    def body(x_ref, wk_ref, wv_ref, *rest):
        outs, w_out, buf = rest[:-2], rest[-2], rest[-1]
        me = lax.axis_index("sp")
        turned = x_ref[...].T
        for j in range(dp_count):
            for d in range(sp_count):
                start = (j * sp_count + d) * share
                buf[d, j * share : (j + 1) * share, :] = turned[start : start + share, :]
        for k, out in enumerate(outs):
            out[...] = buf[me ^ k]
        for h in range(kv_width // HEAD_CHANNELS):
            cols = slice(h * HEAD_CHANNELS, (h + 1) * HEAD_CHANNELS)
            w_out[:, 2 * h * HEAD_CHANNELS : 2 * (h + 1) * HEAD_CHANNELS] = jnp.concatenate(
                [wk_ref[:, cols], wv_ref[:, cols]], axis=1
            )

    outs = kernel_call(
        body,
        [shape_of((feats, rows))] * sp_count + [shape_of((w_rows, 2 * kv_width))],
        [pltpu.VMEM((sp_count, feats, rows), bf16)],
        (token_in, key_matrix, value_matrix),
        name="pack_features",
    )
    return outs[:-1], outs[-1]


def angle_tables(token_length):
    half_pairs = HEAD_CHANNELS // 4
    inv_freq = rope_base ** (-np.arange(half_pairs, dtype=np.float64) / half_pairs)
    inv_freq = inv_freq.astype(np.float32)
    channel = np.arange(2 * HEAD_CHANNELS)
    freq = inv_freq[(channel % HEAD_CHANNELS // 2) % half_pairs]
    sign = np.where(channel % 2 == 0, -1.0, 1.0).astype(np.float32)
    tables = []
    for count in (token_length // GRID, GRID):
        angles = (np.arange(count, dtype=np.float32)[:, None] * freq).astype(np.float64)
        tables += [np.cos(angles).astype(np.float32), (np.sin(angles) * sign).astype(np.float32)]
    return tables


def attention(pieces, query_gain, key_gain, sp_count, heads):
    rows, width = pieces[0].shape
    tokens = rows * sp_count
    pair = 2 * HEAD_CHANNELS
    q_width = heads * HEAD_CHANNELS
    chunks = q_width // pair
    tables = angle_tables(tokens)
    q_block = min(256, tokens)

    def body(*refs):
        piece_refs = refs[:sp_count]
        qg_ref, kg_ref, row_cos, row_sin, col_cos, col_sin = refs[sp_count : sp_count + 6]
        outs = refs[sp_count + 6 : 2 * sp_count + 6]
        p_out = refs[2 * sp_count + 6]
        tok, qh, gh, kr, vv, inv_sc, dq_sc, dkv_sc, dq_out = refs[2 * sp_count + 7 :]
        me = lax.axis_index("sp")
        for k in range(sp_count):
            start = pl.multiple_of((me ^ k) * rows, rows)
            tok[pl.ds(start, rows), :] = piece_refs[k][...]
        lane = lax.broadcasted_iota(jnp.int32, (GRID, pair), 1)
        even = lane % 2 == 0
        by_row = lane % HEAD_CHANNELS < HEAD_CHANNELS // 2
        first_head = lane < HEAD_CHANNELS
        seg_r = lax.broadcasted_iota(jnp.int32, (2 * pair, pair), 0) // HEAD_CHANNELS % 2
        seg_c = lax.broadcasted_iota(jnp.int32, (2 * pair, pair), 1) // HEAD_CHANNELS
        seg = jnp.where(seg_r == seg_c, 1.0 / HEAD_CHANNELS, 0.0).astype(bf16)
        q_gain = jnp.concatenate([qg_ref[...], qg_ref[...]], axis=1)
        k_gain = jnp.concatenate([kg_ref[...], kg_ref[...]], axis=1)

        def head_mean(product_f):
            high = product_f.astype(bf16)
            low = (product_f - high.astype(f32)).astype(bf16)
            return dot(jnp.concatenate([high, low], axis=1), seg, 1, 0)

        def swap(value):
            return jnp.where(even, pltpu.roll(value, pair - 1, 1), pltpu.roll(value, 1, 1))

        def angles_of(r):
            cos = jnp.where(by_row, row_cos[r : r + 1, :], col_cos[...])
            sin = jnp.where(by_row, row_sin[r : r + 1, :], col_sin[...])
            return cos, sin

        for r in range(tokens // GRID):
            at = slice(r * GRID, (r + 1) * GRID)
            cos, sin = angles_of(r)
            for c in range(chunks + 1):
                lo = c * pair if c < chunks else 2 * q_width
                raw = tok[at, lo : lo + pair]
                value = raw.astype(f32)
                inv = lax.rsqrt(head_mean(value * value) + norm_eps)
                inv_sc[at, c * pair : (c + 1) * pair] = inv
                normed = value * inv * (q_gain if c < chunks else k_gain)
                turned = (normed * cos + swap(normed) * sin).astype(bf16)
                if c < chunks:
                    grad = tok[at, q_width + lo : q_width + lo + pair]
                    for u in range(2):
                        part = slice(u * HEAD_CHANNELS, (u + 1) * HEAD_CHANNELS)
                        qh[2 * c + u, at, :] = turned[:, part]
                        gh[2 * c + u, at, :] = grad[:, part]
                else:
                    kr[at, :] = turned[:, :HEAD_CHANNELS]
                    vv[at, :] = raw[:, HEAD_CHANNELS:]

        key_rot = kr[...]
        value_in = vv[...]
        key_acc = None
        for h in range(heads):
            for b in range(tokens // q_block):
                at = slice(b * q_block, (b + 1) * q_block)
                query = qh[h, at, :]
                grad = gh[h, at, :]
                scores = dot(key_rot, query, 1, 1)
                top = jnp.max(scores, axis=0, keepdims=True)
                expo = jnp.exp((scores - top) * score_scale)
                prob = expo * (1.0 / jnp.sum(expo, axis=0, keepdims=True))
                prob_grad = dot(value_in, grad, 1, 1)
                row_dot = jnp.sum(prob * prob_grad, axis=0, keepdims=True)
                score_grad = (prob * (prob_grad - row_dot)).astype(bf16)
                prob_low = prob.astype(bf16)
                dv = dot(prob_low, grad, 1, 0)
                dk = dot(score_grad, query, 1, 0)
                dq_t = dot(key_rot, score_grad, 0, 0)
                dq_sc[at, h * HEAD_CHANNELS : (h + 1) * HEAD_CHANNELS] = dq_t.T * score_scale
                key_acc = dk if key_acc is None else key_acc + dk
                value_acc = dv if h == 0 and b == 0 else value_acc + dv
        dkv_sc[...] = jnp.concatenate([key_acc * score_scale, value_acc], axis=1)

        for r in range(tokens // GRID):
            at = slice(r * GRID, (r + 1) * GRID)
            cos, sin = angles_of(r)
            for c in range(chunks + 1):
                lo = c * pair if c < chunks else 2 * q_width
                value = tok[at, lo : lo + pair].astype(f32)
                inv = inv_sc[at, c * pair : (c + 1) * pair]
                grad = dq_sc[at, lo : lo + pair] if c < chunks else dkv_sc[at, :]
                weighted = (grad * cos - swap(grad) * sin) * (q_gain if c < chunks else k_gain)
                inner = head_mean(weighted * value)
                result = inv * (weighted - value * inv * inv * inner)
                if c < chunks:
                    dq_out[at, lo : lo + pair] = result.astype(bf16)
                else:
                    p_out[at, :] = jnp.where(first_head, result, grad).astype(bf16)
        for k in range(sp_count):
            start = pl.multiple_of((me ^ k) * rows, rows)
            outs[k][...] = dq_out[pl.ds(start, rows), :]

    outs = kernel_call(
        body,
        [shape_of((rows, q_width))] * sp_count + [shape_of((tokens, pair))],
        [
            pltpu.VMEM((tokens, width), bf16),
            pltpu.VMEM((heads, tokens, HEAD_CHANNELS), bf16),
            pltpu.VMEM((heads, tokens, HEAD_CHANNELS), bf16),
            pltpu.VMEM((tokens, HEAD_CHANNELS), bf16),
            pltpu.VMEM((tokens, HEAD_CHANNELS), bf16),
            pltpu.VMEM((tokens, (chunks + 1) * pair), f32),
            pltpu.VMEM((tokens, q_width), f32),
            pltpu.VMEM((tokens, pair), f32),
            pltpu.VMEM((tokens, q_width), bf16),
        ],
        (*pieces, query_gain[None], key_gain[None], *[jnp.asarray(t) for t in tables]),
        flops=10 * heads * tokens * tokens * HEAD_CHANNELS,
        name="attention",
    )
    return outs[:-1], outs[-1]


def weight_partials(turned_pieces, grad_pieces, sp_count, dp_count):
    feats, rows = turned_pieces[0].shape
    tokens, pair = grad_pieces[0].shape
    share = feats // dp_count

    def body(*refs):
        x_refs, p_refs = refs[:sp_count], refs[sp_count : 2 * sp_count]
        outs = refs[2 * sp_count : 2 * sp_count + dp_count]
        x_all, p_all, buf = refs[2 * sp_count + dp_count :]
        me = lax.axis_index("sp")
        mine = lax.axis_index("dp")
        for k in range(sp_count):
            x_all[:, k * rows : (k + 1) * rows] = x_refs[k][...]
            start = pl.multiple_of((me ^ k) * rows, rows)
            for c in range(sp_count):
                p_all[k * rows : (k + 1) * rows, c * pair : (c + 1) * pair] = p_refs[c][
                    pl.ds(start, rows), :
                ]
        result = dot(x_all[...], p_all[...], 1, 0).astype(bf16)
        for c in range(sp_count):
            for j in range(dp_count):
                buf[j, me ^ c] = result[j * share : (j + 1) * share, c * pair : (c + 1) * pair]
        for m, out in enumerate(outs):
            out[...] = buf[mine ^ m]

    return kernel_call(
        body,
        [shape_of((sp_count, share, pair))] * dp_count,
        [
            pltpu.VMEM((feats, tokens), bf16),
            pltpu.VMEM((tokens, sp_count * pair), bf16),
            pltpu.VMEM((dp_count, sp_count, share, pair), bf16),
        ],
        (*turned_pieces, *grad_pieces),
        flops=2 * feats * tokens * sp_count * pair,
        name="weight_partials",
    )


def sum_pieces(pieces):
    def body(*refs):
        total = refs[0][...].astype(f32)
        for ref in refs[1:-1]:
            total = total + ref[...].astype(f32)
        refs[-1][...] = total.astype(bf16)

    return kernel_call(body, shape_of(pieces[0].shape), [], tuple(pieces), name="sum_pieces")


def join_weight_grads(pieces, sp_count):
    groups, share, pair = pieces[0].shape
    half = pair // 2
    rows = share * sp_count

    def body(*refs):
        k_out, v_out = refs[sp_count:]
        me = lax.axis_index("sp")
        for k in range(sp_count):
            start = pl.multiple_of((me ^ k) * share, share)
            block = refs[k][...].astype(f32)
            k_out[pl.ds(start, share), :] = jnp.concatenate(
                [block[h, :, :half] for h in range(groups)], axis=1
            )
            v_out[pl.ds(start, share), :] = jnp.concatenate(
                [block[h, :, half:] for h in range(groups)], axis=1
            )

    return kernel_call(
        body, [shape_of((rows, groups * half), f32)] * 2, [], tuple(pieces), name="join_weight_grads"
    )


def input_gradient(grad_pieces, weight_pieces, rows, sp_count, dp_count):
    pair = grad_pieces[0].shape[1]
    w_rows = weight_pieces[0].shape[0]

    def body(*refs):
        p_refs, w_refs = refs[:sp_count], refs[sp_count : sp_count + dp_count]
        out, p_buf, out_buf = refs[sp_count + dp_count :]
        me = lax.axis_index("sp")
        mine = lax.axis_index("dp")
        start = pl.multiple_of(me * rows, rows)
        for k in range(sp_count):
            p_buf[me ^ k] = p_refs[k][pl.ds(start, rows), :]
        left = jnp.concatenate([p_buf[h] for h in range(sp_count)], axis=1)
        for m in range(dp_count):
            out_buf[mine ^ m] = dot(left, w_refs[m][...], 1, 1).astype(bf16)
        for j in range(dp_count):
            out[:, j * w_rows : (j + 1) * w_rows] = out_buf[j]

    return kernel_call(
        body,
        shape_of((rows, dp_count * w_rows)),
        [pltpu.VMEM((sp_count, rows, pair), bf16), pltpu.VMEM((dp_count, rows, w_rows), bf16)],
        (*grad_pieces, *weight_pieces),
        flops=2 * rows * dp_count * w_rows * sp_count * pair,
        name="input_gradient",
    )


def join_query_grads(pieces, sp_count):
    rows, width = pieces[0].shape

    def body(*refs):
        out, buf = refs[sp_count:]
        me = lax.axis_index("sp")
        for k in range(sp_count):
            buf[me ^ k] = refs[k][...]
        for d in range(sp_count):
            out[:, d * width : (d + 1) * width] = buf[d]

    return kernel_call(
        body,
        shape_of((rows, sp_count * width)),
        [pltpu.VMEM((sp_count, rows, width), bf16)],
        tuple(pieces),
        name="join_query_grads",
    )


def fast_device(
    inputs, queries, keys, values, out_grad, query_gain, key_gain, key_matrix, value_matrix
):
    sp_count = lax.axis_size("sp")
    dp_count = lax.axis_size("dp")
    rows = inputs.shape[1]
    heads = QUERY_HEADS // sp_count
    sp_order = list(range(1, sp_count))[::-1]
    dp_order = list(range(1, dp_count))[::-1]
    packed = pack_heads(queries[0], keys[0], values[0], out_grad[0], sp_count)
    head_pieces = exchange(packed, "sp", sp_order)
    turned, joined_weight = pack_features(
        inputs[0], key_matrix, value_matrix, sp_count, dp_count
    )
    turned_pieces = exchange(turned, "sp", sp_order)
    weight_pieces = exchange([joined_weight] * dp_count, "dp", dp_order)
    query_parts, grad_part = attention(head_pieces, query_gain, key_gain, sp_count, heads)
    grad_pieces = exchange([grad_part] * sp_count, "sp", sp_order)
    query_pieces = exchange(query_parts, "sp", sp_order)
    partials = weight_partials(turned_pieces, grad_pieces, sp_count, dp_count)
    summed = sum_pieces(exchange(partials, "dp", dp_order))
    input_grad = input_gradient(grad_pieces, weight_pieces, rows, sp_count, dp_count)
    query_grad = join_query_grads(query_pieces, sp_count)
    key_weight, value_weight = join_weight_grads(
        exchange([summed] * sp_count, "sp", sp_order), sp_count
    )
    return input_grad[None], query_grad[None], key_weight, value_weight


def choose_device(mesh):
    sp_count, dp_count = mesh.shape["sp"], mesh.shape["dp"]
    powers = sp_count & (sp_count - 1) == 0 and dp_count & (dp_count - 1) == 0
    return fast_device if powers and sp_count == KEY_VALUE_HEADS else generic_device


def solution(mesh):
    return jax.shard_map(
        choose_device(mesh),
        mesh=mesh,
        in_specs=(
            P("dp", "sp", None),
            P("dp", "sp", None),
            P("dp", "sp", None),
            P("dp", "sp", None),
            P("dp", "sp", None),
            P(),
            P(),
            P("dp", None),
            P("dp", None),
        ),
        out_specs=(P("dp", "sp", None), P("dp", "sp", None), P("dp", None), P("dp", None)),
        check_vma=False,
    )
```

```python
import jax
import jax.numpy as jnp
import numpy as np
from jax import lax
from jax.experimental import pallas as pl
from jax.experimental.pallas import tpu as pltpu
from jax.sharding import PartitionSpec as P

QUERY_HEADS = 16
KEY_VALUE_HEADS = 4
HEAD_CHANNELS = 64
GRID = 64


rope_base = 10000.0
norm_eps = 0.5
score_scale = 0.125


def product(pattern, first_op, second_op):
    return jnp.einsum(pattern, first_op, second_op, preferred_element_type=jnp.float32)


def rotary_tables(token_length):
    position = jnp.arange(token_length, dtype=jnp.int32)
    grid_row = (position // GRID).astype(jnp.float32)
    grid_col = (position % GRID).astype(jnp.float32)
    half_pairs = HEAD_CHANNELS // 4
    inv_freq = rope_base ** (-jnp.arange(half_pairs, dtype=jnp.float32) / half_pairs)
    angles = jnp.concatenate([grid_row[:, None] * inv_freq, grid_col[:, None] * inv_freq], axis=1)
    return (jnp.cos(angles), jnp.sin(angles))


def rotate(vector, cos_tab, sin_tab):
    even_part = vector[..., 0::2]
    odd_part = vector[..., 1::2]
    turned = jnp.stack(
        [even_part * cos_tab - odd_part * sin_tab, even_part * sin_tab + odd_part * cos_tab],
        axis=-1,
    )
    return turned.reshape(vector.shape)


def rotate_back(cotangent, cos_tab, sin_tab):
    even_part = cotangent[..., 0::2]
    odd_part = cotangent[..., 1::2]
    turned = jnp.stack(
        [even_part * cos_tab + odd_part * sin_tab, odd_part * cos_tab - even_part * sin_tab],
        axis=-1,
    )
    return turned.reshape(cotangent.shape)


def inverse_rms(vector):
    return lax.rsqrt(jnp.mean(vector * vector, axis=-1, keepdims=True) + norm_eps)


def norm_back(vector, inv_scale, cotangent, gain_vec):
    weighted = cotangent * gain_vec
    inner_mean = jnp.mean(weighted * vector, axis=-1, keepdims=True)
    return inv_scale * (weighted - vector * inv_scale * inv_scale * inner_mean)


def head_grads(
    query_in, key_input, value_input, grad_in, query_gain, key_gain, cos_tab, sin_tab, block_rows
):
    token_length, groups, per_group, head_dim = query_in.shape
    cos_four = cos_tab[:, None, None, :]
    sin_four = sin_tab[:, None, None, :]
    cos_three = cos_tab[:, None, :]
    sin_three = sin_tab[:, None, :]
    query_f = query_in.astype(jnp.float32)
    query_inv = inverse_rms(query_f)
    query_rot = rotate(query_f * query_inv * query_gain, cos_four, sin_four).astype(jnp.bfloat16)
    key_f = key_input.astype(jnp.float32)
    key_inv = inverse_rms(key_f)
    key_rot = rotate(key_f * key_inv * key_gain, cos_three, sin_three).astype(jnp.bfloat16)
    num_blocks = token_length // block_rows
    query_blocks = query_rot.reshape(num_blocks, block_rows, groups, per_group, head_dim)
    grad_blocks = grad_in.reshape(num_blocks, block_rows, groups, per_group, head_dim)

    def attend_block(carried, pieces):
        key_acc, value_acc = carried
        query_piece, grad_piece = pieces
        scores = product("qgrd,cgd->grqc", query_piece, key_rot) * score_scale
        row_max = jnp.max(scores, axis=-1, keepdims=True)
        shifted = jnp.exp(scores - row_max)
        attn_prob = shifted / jnp.sum(shifted, axis=-1, keepdims=True)
        prob_low = attn_prob.astype(jnp.bfloat16)
        prob_grad = product("qgrd,cgd->grqc", grad_piece, value_input)
        row_dot = jnp.sum(attn_prob * prob_grad, axis=-1, keepdims=True)
        score_grad = (attn_prob * (prob_grad - row_dot) * score_scale).astype(jnp.bfloat16)
        dq_piece = product("grqc,cgd->qgrd", score_grad, key_rot)
        key_acc = key_acc + product("grqc,qgrd->cgd", score_grad, query_piece)
        value_acc = value_acc + product("grqc,qgrd->cgd", prob_low, grad_piece)
        return ((key_acc, value_acc), dq_piece)

    empty_acc = jnp.zeros((token_length, groups, head_dim), jnp.float32)
    (key_rot_grad, value_acc), query_rot_grad = lax.scan(
        attend_block, (empty_acc, empty_acc), (query_blocks, grad_blocks)
    )
    query_rot_grad = query_rot_grad.reshape(token_length, groups, per_group, head_dim)
    query_grad = norm_back(
        query_f, query_inv, rotate_back(query_rot_grad, cos_four, sin_four), query_gain
    ).astype(jnp.bfloat16)
    key_portion = norm_back(
        key_f, key_inv, rotate_back(key_rot_grad, cos_three, sin_three), key_gain
    ).astype(jnp.bfloat16)
    return (query_grad, key_portion, value_acc.astype(jnp.bfloat16))


def generic_device(
    inputs, queries, keys, values, out_grad, query_gain, key_gain, key_matrix, value_matrix
):
    sp_count = lax.axis_size("sp")
    dp_count = lax.axis_size("dp")
    token_row_block = inputs.shape[1]
    token_length = token_row_block * sp_count
    local_heads = QUERY_HEADS // sp_count
    portion_heads = min(local_heads, QUERY_HEADS // KEY_VALUE_HEADS)
    kv_here = local_heads // portion_heads
    group_copies = QUERY_HEADS // KEY_VALUE_HEADS // portion_heads
    key_value_width = KEY_VALUE_HEADS * HEAD_CHANNELS
    key_positions = jnp.repeat(
        keys[0].reshape(token_row_block, KEY_VALUE_HEADS, HEAD_CHANNELS), group_copies, axis=1
    ).reshape(token_row_block, key_value_width * group_copies)
    value_positions = jnp.repeat(
        values[0].reshape(token_row_block, KEY_VALUE_HEADS, HEAD_CHANNELS), group_copies, axis=1
    ).reshape(token_row_block, key_value_width * group_copies)
    grad_heads, query_heads, key_heads, value_heads = (
        lax.all_to_all(out_grad[0], "sp", split_axis=1, concat_axis=0, tiled=True),
        lax.all_to_all(queries[0], "sp", split_axis=1, concat_axis=0, tiled=True),
        lax.all_to_all(key_positions, "sp", split_axis=1, concat_axis=0, tiled=True),
        lax.all_to_all(value_positions, "sp", split_axis=1, concat_axis=0, tiled=True),
    )
    cos_tab, sin_tab = rotary_tables(token_length)
    query_part, key_portion, value_portion = head_grads(
        query_heads.reshape(token_length, kv_here, portion_heads, HEAD_CHANNELS),
        key_heads.reshape(token_length, kv_here, HEAD_CHANNELS),
        value_heads.reshape(token_length, kv_here, HEAD_CHANNELS),
        grad_heads.reshape(token_length, kv_here, portion_heads, HEAD_CHANNELS),
        query_gain,
        key_gain,
        cos_tab,
        sin_tab,
        min(512, token_length),
    )
    query_tokens, key_token_rows, value_token_rows = (
        lax.all_to_all(
            query_part.reshape(token_length, local_heads * HEAD_CHANNELS),
            "sp",
            split_axis=0,
            concat_axis=1,
            tiled=True,
        ),
        lax.all_to_all(
            key_portion.reshape(token_length, kv_here * HEAD_CHANNELS),
            "sp",
            split_axis=0,
            concat_axis=1,
            tiled=True,
        ),
        lax.all_to_all(
            value_portion.reshape(token_length, kv_here * HEAD_CHANNELS),
            "sp",
            split_axis=0,
            concat_axis=1,
            tiled=True,
        ),
    )
    key_gradient = (
        key_token_rows.reshape(token_row_block, KEY_VALUE_HEADS, group_copies, HEAD_CHANNELS)
        .astype(jnp.float32)
        .sum(axis=2)
        .astype(jnp.bfloat16)
    )
    value_gradient = (
        value_token_rows.reshape(token_row_block, KEY_VALUE_HEADS, group_copies, HEAD_CHANNELS)
        .astype(jnp.float32)
        .sum(axis=2)
        .astype(jnp.bfloat16)
    )
    projection_gradient = jnp.concatenate(
        [
            key_gradient.reshape(token_row_block, key_value_width),
            value_gradient.reshape(token_row_block, key_value_width),
        ],
        axis=1,
    )
    joined_weight = jnp.concatenate([key_matrix, value_matrix], axis=1)
    input_grad = lax.dot_general(
        projection_gradient,
        lax.all_gather(joined_weight, "dp", axis=0, tiled=True),
        (((1,), (1,)), ((), ())),
        preferred_element_type=jnp.float32,
    ).astype(jnp.bfloat16)
    token_in = inputs[0]
    width = inputs.shape[2]
    row_share = width // (sp_count * dp_count)
    permuted = (
        token_in.reshape(token_row_block, dp_count, sp_count, row_share)
        .transpose(0, 2, 1, 3)
        .reshape(token_row_block, width)
    )
    share_cols = lax.all_to_all(permuted, "sp", split_axis=1, concat_axis=0, tiled=True)
    all_grads = lax.all_gather(projection_gradient, "sp", axis=0, tiled=True)
    grad_piece = lax.psum_scatter(
        lax.dot_general(
            share_cols, all_grads, (((0,), (0,)), ((), ())), preferred_element_type=jnp.float32
        ).astype(jnp.bfloat16),
        "dp",
        scatter_dimension=0,
        tiled=True,
    ).astype(jnp.float32)
    weight_grad = lax.all_gather(grad_piece, "sp", axis=0, tiled=True)
    return (
        input_grad[None],
        query_tokens[None],
        weight_grad[:, :key_value_width],
        weight_grad[:, key_value_width:],
    )


bf16 = jnp.bfloat16
f32 = jnp.float32


def dot(first_op, second_op, first_dim, second_dim):
    return lax.dot_general(
        first_op, second_op, (((first_dim,), (second_dim,)), ((), ())), preferred_element_type=f32
    )


def kernel_call(body, out_shape, scratch, args, flops=0):
    vmem = pl.BlockSpec(memory_space=pltpu.VMEM)
    return pl.pallas_call(
        body,
        out_shape=out_shape,
        in_specs=[vmem] * len(args),
        out_specs=jax.tree.map(lambda _: vmem, out_shape),
        scratch_shapes=scratch,
        cost_estimate=pl.CostEstimate(flops=flops, bytes_accessed=0, transcendentals=0),
        compiler_params=pltpu.CompilerParams(vmem_limit_bytes=58 * 1024 * 1024),
    )(*args)


def shape_of(shape, dtype=bf16):
    return jax.ShapeDtypeStruct(shape, dtype)


def swap_with(value, axis, k):
    count = lax.axis_size(axis)
    return lax.ppermute(value, axis, [(i, i ^ k) for i in range(count)])


def pack_heads(queries, keys, values, out_grad):
    rows, q_all = queries.shape
    kv_half = keys.shape[1] // 2
    q_half = q_all // 2
    width = 2 * q_half + 2 * kv_half

    def body(q_ref, g_ref, k_ref, v_ref, own, mate, far, far_mate, buf):
        bit = lax.axis_index("sp") % 2
        for d in range(2):
            buf[d, :, :q_half] = q_ref[:, d * q_half : (d + 1) * q_half]
            buf[d, :, q_half : 2 * q_half] = g_ref[:, d * q_half : (d + 1) * q_half]
            parts = []
            for h in range(kv_half // HEAD_CHANNELS):
                lo = d * kv_half + h * HEAD_CHANNELS
                parts += [k_ref[:, lo : lo + HEAD_CHANNELS], v_ref[:, lo : lo + HEAD_CHANNELS]]
            buf[d, :, 2 * q_half :] = jnp.concatenate(parts, axis=1)
        own[...] = buf[bit]
        mate[...] = buf[1 - bit]
        far[...] = buf[bit, :, 2 * q_half :]
        far_mate[...] = buf[1 - bit, :, 2 * q_half :]

    return kernel_call(
        body,
        [shape_of((rows, width))] * 2 + [shape_of((rows, 2 * kv_half))] * 2,
        [pltpu.VMEM((2, rows, width), bf16)],
        (queries, out_grad, keys, values),
    )


def join_weights(key_matrix, value_matrix):
    rows, kv_width = key_matrix.shape

    def body(wk_ref, wv_ref, out):
        for h in range(kv_width // HEAD_CHANNELS):
            cols = slice(h * HEAD_CHANNELS, (h + 1) * HEAD_CHANNELS)
            out[:, 2 * h * HEAD_CHANNELS : 2 * (h + 1) * HEAD_CHANNELS] = jnp.concatenate(
                [wk_ref[:, cols], wv_ref[:, cols]], axis=1
            )

    return kernel_call(body, shape_of((rows, 2 * kv_width)), [], (key_matrix, value_matrix))


def turn_inputs(token_in):
    def body(x_ref, out):
        out[...] = x_ref[...].T

    return kernel_call(body, shape_of(token_in.shape[::-1]), [], (token_in,))


def angle_tables(token_length):
    half_pairs = HEAD_CHANNELS // 4
    inv_freq = rope_base ** (-np.arange(half_pairs, dtype=np.float64) / half_pairs)
    inv_freq = inv_freq.astype(np.float32)
    channel = np.arange(2 * HEAD_CHANNELS)
    freq = inv_freq[(channel % HEAD_CHANNELS // 2) % half_pairs]
    sign = np.where(channel % 2 == 0, -1.0, 1.0).astype(np.float32)
    tables = []
    for count in (token_length // GRID, GRID):
        angles = (np.arange(count, dtype=np.float32)[:, None] * freq).astype(np.float64)
        tables += [np.cos(angles).astype(np.float32), (np.sin(angles) * sign).astype(np.float32)]
    return tables


def attention(own, mate, far, far_mate, query_gain, key_gain):
    rows, width = own.shape
    kv_width = far.shape[1]
    q_width = (width - kv_width) // 2
    pair = 2 * HEAD_CHANNELS
    heads = q_width // HEAD_CHANNELS
    groups = kv_width // pair
    per_group = heads // groups
    q_chunks = q_width // pair
    half = 2 * rows
    tokens = 4 * rows
    tables = angle_tables(tokens)

    def body(*refs):
        own_ref, mate_ref, far_ref, far_mate_ref, qg_ref, kg_ref = refs[:6]
        row_cos, row_sin, col_cos, col_sin = refs[6:10]
        dq_own, dq_mate, p_own, p_far = refs[10:14]
        q_tok, kv_tok, qh, gh, kr, vv, q_inv, k_inv, dq_sc, dkv_sc, dq_out, p_sc = refs[14:]
        me = lax.axis_index("sp")
        bit = me % 2
        upper = me // 2
        q_own = pl.multiple_of(bit * rows, rows)
        q_mate = pl.multiple_of((1 - bit) * rows, rows)
        q_tok[pl.ds(q_own, rows), :] = own_ref[:, : 2 * q_width]
        q_tok[pl.ds(q_mate, rows), :] = mate_ref[:, : 2 * q_width]
        for k, block in enumerate(
            (own_ref[:, 2 * q_width :], mate_ref[:, 2 * q_width :], far_ref[...], far_mate_ref[...])
        ):
            kv_tok[pl.ds(pl.multiple_of((me ^ k) * rows, rows), rows), :] = block
        lane = lax.broadcasted_iota(jnp.int32, (GRID, pair), 1)
        even = lane % 2 == 0
        by_row = lane % HEAD_CHANNELS < HEAD_CHANNELS // 2
        first_head = lane < HEAD_CHANNELS
        seg_r = lax.broadcasted_iota(jnp.int32, (2 * pair, pair), 0) // HEAD_CHANNELS % 2
        seg_c = lax.broadcasted_iota(jnp.int32, (2 * pair, pair), 1) // HEAD_CHANNELS
        seg = jnp.where(seg_r == seg_c, 1.0 / HEAD_CHANNELS, 0.0).astype(bf16)
        q_gain = jnp.concatenate([qg_ref[...], qg_ref[...]], axis=1)
        k_gain = jnp.concatenate([kg_ref[...], kg_ref[...]], axis=1)

        def head_mean(product_f):
            high = product_f.astype(bf16)
            low = (product_f - high.astype(f32)).astype(bf16)
            return dot(jnp.concatenate([high, low], axis=1), seg, 1, 0)

        def swap(value):
            return jnp.where(even, pltpu.roll(value, pair - 1, 1), pltpu.roll(value, 1, 1))

        def angles_of(r):
            cos = jnp.where(by_row, row_cos[pl.ds(r, 1), :], col_cos[...])
            sin = jnp.where(by_row, row_sin[pl.ds(r, 1), :], col_sin[...])
            return cos, sin

        def forward(value, gain, cos, sin):
            inv = lax.rsqrt(head_mean(value * value) + norm_eps)
            normed = value * inv * gain
            return inv, (normed * cos + swap(normed) * sin).astype(bf16)

        def backward(value, inv, grad, gain, cos, sin):
            weighted = (grad * cos - swap(grad) * sin) * gain
            inner = head_mean(weighted * value)
            return inv * (weighted - value * inv * inv * inner)

        q_rows = half // GRID
        for r in range(tokens // GRID):
            at = slice(r * GRID, (r + 1) * GRID)
            cos, sin = angles_of(r)
            for c in range(groups):
                part = slice(c * pair, (c + 1) * pair)
                raw = kv_tok[at, part]
                inv, turned = forward(raw.astype(f32), k_gain, cos, sin)
                k_inv[at, part] = inv
                kr[c, at, :] = turned[:, :HEAD_CHANNELS]
                vv[c, at, :] = raw[:, HEAD_CHANNELS:]
        for r in range(q_rows):
            at = slice(r * GRID, (r + 1) * GRID)
            cos, sin = angles_of(upper * q_rows + r)
            for c in range(q_chunks):
                part = slice(c * pair, (c + 1) * pair)
                inv, turned = forward(q_tok[at, part].astype(f32), q_gain, cos, sin)
                q_inv[at, part] = inv
                grad = q_tok[at, q_width + c * pair : q_width + (c + 1) * pair]
                for u in range(2):
                    lanes = slice(u * HEAD_CHANNELS, (u + 1) * HEAD_CHANNELS)
                    qh[2 * c + u, at, :] = turned[:, lanes]
                    gh[2 * c + u, at, :] = grad[:, lanes]

        for g in range(groups):
            key_rot = kr[g]
            value_in = vv[g]
            for h in range(g * per_group, (g + 1) * per_group):
                query = qh[h]
                grad = gh[h]
                scores = dot(key_rot, query, 1, 1)
                top = jnp.max(scores, axis=0, keepdims=True)
                expo = jnp.exp((scores - top) * score_scale)
                prob = expo * (1.0 / jnp.sum(expo, axis=0, keepdims=True))
                prob_grad = dot(value_in, grad, 1, 1)
                row_dot = jnp.sum(prob * prob_grad, axis=0, keepdims=True)
                score_grad = (prob * (prob_grad - row_dot)).astype(bf16)
                dv = dot(prob.astype(bf16), grad, 1, 0)
                dk = dot(score_grad, query, 1, 0)
                dq_t = dot(key_rot, score_grad, 0, 0)
                dq_sc[:, h * HEAD_CHANNELS : (h + 1) * HEAD_CHANNELS] = dq_t.T * score_scale
                first = h == g * per_group
                key_acc = dk if first else key_acc + dk
                value_acc = dv if first else value_acc + dv
            dkv_sc[:, g * pair : (g + 1) * pair] = jnp.concatenate(
                [key_acc * score_scale, value_acc], axis=1
            )

        for r in range(tokens // GRID):
            at = slice(r * GRID, (r + 1) * GRID)
            cos, sin = angles_of(r)
            for c in range(groups):
                part = slice(c * pair, (c + 1) * pair)
                grad = dkv_sc[at, part]
                value = kv_tok[at, part].astype(f32)
                result = backward(value, k_inv[at, part], grad, k_gain, cos, sin)
                p_sc[at, part] = jnp.where(first_head, result, grad)
        p_own[...] = p_sc[pl.ds(pl.multiple_of(upper * half, half), half), :]
        p_far[...] = p_sc[pl.ds(pl.multiple_of((1 - upper) * half, half), half), :].astype(bf16)
        for r in range(q_rows):
            at = slice(r * GRID, (r + 1) * GRID)
            cos, sin = angles_of(upper * q_rows + r)
            for c in range(q_chunks):
                part = slice(c * pair, (c + 1) * pair)
                value = q_tok[at, part].astype(f32)
                result = backward(value, q_inv[at, part], dq_sc[at, part], q_gain, cos, sin)
                dq_out[at, part] = result.astype(bf16)
        dq_own[...] = dq_out[pl.ds(q_own, rows), :]
        dq_mate[...] = dq_out[pl.ds(q_mate, rows), :]

    return kernel_call(
        body,
        [shape_of((rows, q_width))] * 2
        + [shape_of((half, kv_width), f32), shape_of((half, kv_width))],
        [
            pltpu.VMEM((half, 2 * q_width), bf16),
            pltpu.VMEM((tokens, kv_width), bf16),
            pltpu.VMEM((heads, half, HEAD_CHANNELS), bf16),
            pltpu.VMEM((heads, half, HEAD_CHANNELS), bf16),
            pltpu.VMEM((groups, tokens, HEAD_CHANNELS), bf16),
            pltpu.VMEM((groups, tokens, HEAD_CHANNELS), bf16),
            pltpu.VMEM((half, q_width), f32),
            pltpu.VMEM((tokens, kv_width), f32),
            pltpu.VMEM((half, q_width), f32),
            pltpu.VMEM((tokens, kv_width), f32),
            pltpu.VMEM((half, q_width), bf16),
            pltpu.VMEM((tokens, kv_width), f32),
        ],
        (
            own,
            mate,
            far,
            far_mate,
            query_gain[None],
            key_gain[None],
            *[jnp.asarray(t) for t in tables],
        ),
        flops=10 * heads * half * tokens * HEAD_CHANNELS,
    )


def weight_partials(turned_own, turned_mate, p_own, p_far, dp_count):
    feats, rows = turned_own.shape
    half, cols = p_own.shape
    share = feats // dp_count

    def body(xo_ref, xm_ref, po_ref, pf_ref, *rest):
        mine_out, mate_out = rest[:2]
        outs = rest[2 : 2 + dp_count]
        x_all, p_sc, res = rest[2 + dp_count :]
        bit = lax.axis_index("sp") % 2
        mine = lax.axis_index("dp")
        p_sc[...] = (po_ref[...] + pf_ref[...].astype(f32)).astype(bf16)
        p_mine = p_sc[pl.ds(pl.multiple_of(bit * rows, rows), rows), :]
        p_mate = p_sc[pl.ds(pl.multiple_of((1 - bit) * rows, rows), rows), :]
        mine_out[...] = p_mine
        mate_out[...] = p_mate
        x_all[:, :rows] = xo_ref[...]
        x_all[:, rows:] = xm_ref[...]
        p_all = jnp.concatenate([p_mine, p_mate], axis=0)
        res[...] = dot(x_all[...], p_all, 1, 0).astype(bf16)
        for m, out in enumerate(outs):
            out[...] = res[pl.ds(pl.multiple_of((mine ^ m) * share, share), share), :]

    outs = kernel_call(
        body,
        [shape_of((rows, cols))] * 2 + [shape_of((share, cols))] * dp_count,
        [
            pltpu.VMEM((feats, half), bf16),
            pltpu.VMEM((half, cols), bf16),
            pltpu.VMEM((feats, cols), bf16),
        ],
        (turned_own, turned_mate, p_own, p_far),
        flops=2 * feats * half * cols,
    )
    return outs[0], outs[1], outs[2:]


def sum_pieces(pieces):
    total = pieces[0].astype(f32)
    for piece in pieces[1:]:
        total = total + piece.astype(f32)
    return total.astype(bf16)


def join_weight_grads(own, mate, far, far_mate):
    rows, cols = own.shape
    pair = 2 * HEAD_CHANNELS
    groups = cols // pair

    def body(own_ref, mate_ref, far_ref, far_mate_ref, k_out, v_out, buf):
        bit = lax.axis_index("sp") % 2
        buf[bit] = own_ref[...].astype(f32) + far_ref[...].astype(f32)
        buf[1 - bit] = mate_ref[...].astype(f32) + far_mate_ref[...].astype(f32)
        parts = [buf[d, :, g * pair : (g + 1) * pair] for d in range(2) for g in range(groups)]
        k_out[...] = jnp.concatenate([p[:, :HEAD_CHANNELS] for p in parts], axis=1)
        v_out[...] = jnp.concatenate([p[:, HEAD_CHANNELS:] for p in parts], axis=1)

    return kernel_call(
        body,
        [shape_of((rows, cols), f32)] * 2,
        [pltpu.VMEM((2, rows, cols), f32)],
        (own, mate, far, far_mate),
    )


def token_outputs(p_mine, p_from_mate, weight_pieces, dq_own, dq_from_mate):
    rows, cols = p_mine.shape
    q_half = dq_own.shape[1]
    dp_count = len(weight_pieces)
    w_rows = weight_pieces[0].shape[0]

    def body(p_ref, pm_ref, dq_ref, dqm_ref, *rest):
        w_refs = rest[:dp_count]
        x_out, q_out, p_buf, out_buf, q_buf = rest[dp_count:]
        bit = lax.axis_index("sp") % 2
        mine = lax.axis_index("dp")
        p_buf[bit] = p_ref[...]
        p_buf[1 - bit] = pm_ref[...]
        q_buf[bit] = dq_ref[...]
        q_buf[1 - bit] = dqm_ref[...]
        for d in range(2):
            q_out[:, d * q_half : (d + 1) * q_half] = q_buf[d]
        left = jnp.concatenate([p_buf[0], p_buf[1]], axis=1)
        for m in range(dp_count):
            out_buf[mine ^ m] = dot(left, w_refs[m][...], 1, 1).astype(bf16)
        for j in range(dp_count):
            x_out[:, j * w_rows : (j + 1) * w_rows] = out_buf[j]

    return kernel_call(
        body,
        [shape_of((rows, dp_count * w_rows)), shape_of((rows, 2 * q_half))],
        [
            pltpu.VMEM((2, rows, cols), bf16),
            pltpu.VMEM((dp_count, rows, w_rows), bf16),
            pltpu.VMEM((2, rows, q_half), bf16),
        ],
        (p_mine, p_from_mate, dq_own, dq_from_mate, *weight_pieces),
        flops=4 * rows * dp_count * w_rows * cols,
    )


def fast_device(
    inputs, queries, keys, values, out_grad, query_gain, key_gain, key_matrix, value_matrix
):
    return fast_body(
        inputs[0],
        queries[0],
        keys[0],
        values[0],
        out_grad[0],
        query_gain,
        key_gain,
        key_matrix,
        value_matrix,
    )


def fast_body(
    inputs, queries, keys, values, out_grad, query_gain, key_gain, key_matrix, value_matrix
):
    others = range(1, lax.axis_size("dp"))
    own, mate, far, far_mate = pack_heads(queries, keys, values, out_grad)
    mate = swap_with(mate, "sp", 1)
    far = swap_with(far, "sp", 2)
    far_mate = swap_with(far_mate, "sp", 3)
    joined_weight = join_weights(key_matrix, value_matrix)
    weight_pieces = [joined_weight] + [swap_with(joined_weight, "dp", m) for m in others]
    turned = turn_inputs(inputs)
    turned_mate = swap_with(turned, "sp", 1)
    dq_own, dq_mate, p_own, p_far = attention(own, mate, far, far_mate, query_gain, key_gain)
    p_far = swap_with(p_far, "sp", 2)
    dq_mate = swap_with(dq_mate, "sp", 1)
    p_mine, p_mate, partials = weight_partials(
        turned, turned_mate, p_own, p_far, lax.axis_size("dp")
    )
    p_mate = swap_with(p_mate, "sp", 1)
    summed = sum_pieces([partials[0]] + [swap_with(partials[m], "dp", m) for m in others])
    input_grad, query_grad = token_outputs(p_mine, p_mate, weight_pieces, dq_own, dq_mate)
    key_weight, value_weight = join_weight_grads(
        summed, *[swap_with(summed, "sp", k) for k in range(1, 4)]
    )
    return input_grad[None], query_grad[None], key_weight, value_weight


def solution(mesh):
    sp_count, dp_count = mesh.shape["sp"], mesh.shape["dp"]
    fast = sp_count == 4 and dp_count & (dp_count - 1) == 0
    return jax.shard_map(
        fast_device if fast else generic_device,
        mesh=mesh,
        in_specs=(
            P("dp", "sp", None),
            P("dp", "sp", None),
            P("dp", "sp", None),
            P("dp", "sp", None),
            P("dp", "sp", None),
            P(),
            P(),
            P("dp", None),
            P("dp", None),
        ),
        out_specs=(P("dp", "sp", None), P("dp", "sp", None), P("dp", None), P("dp", None)),
        check_vma=False,
    )
```

```python
import jax
import jax.numpy as jnp
import numpy as np
from jax import lax
from jax.experimental import pallas as pl
from jax.experimental.pallas import tpu as pltpu
from jax.sharding import PartitionSpec as P

QUERY_HEADS = 16
KEY_VALUE_HEADS = 4
HEAD_CHANNELS = 64
GRID = 64


rope_base = 10000.0
norm_eps = 0.5
score_scale = 0.125


def product(pattern, first_op, second_op):
    return jnp.einsum(pattern, first_op, second_op, preferred_element_type=jnp.float32)


def rotary_tables(token_length):
    position = jnp.arange(token_length, dtype=jnp.int32)
    grid_row = (position // GRID).astype(jnp.float32)
    grid_col = (position % GRID).astype(jnp.float32)
    half_pairs = HEAD_CHANNELS // 4
    inv_freq = rope_base ** (-jnp.arange(half_pairs, dtype=jnp.float32) / half_pairs)
    angles = jnp.concatenate([grid_row[:, None] * inv_freq, grid_col[:, None] * inv_freq], axis=1)
    return (jnp.cos(angles), jnp.sin(angles))


def rotate(vector, cos_tab, sin_tab):
    even_part = vector[..., 0::2]
    odd_part = vector[..., 1::2]
    turned = jnp.stack(
        [even_part * cos_tab - odd_part * sin_tab, even_part * sin_tab + odd_part * cos_tab],
        axis=-1,
    )
    return turned.reshape(vector.shape)


def rotate_back(cotangent, cos_tab, sin_tab):
    even_part = cotangent[..., 0::2]
    odd_part = cotangent[..., 1::2]
    turned = jnp.stack(
        [even_part * cos_tab + odd_part * sin_tab, odd_part * cos_tab - even_part * sin_tab],
        axis=-1,
    )
    return turned.reshape(cotangent.shape)


def inverse_rms(vector):
    return lax.rsqrt(jnp.mean(vector * vector, axis=-1, keepdims=True) + norm_eps)


def norm_back(vector, inv_scale, cotangent, gain_vec):
    weighted = cotangent * gain_vec
    inner_mean = jnp.mean(weighted * vector, axis=-1, keepdims=True)
    return inv_scale * (weighted - vector * inv_scale * inv_scale * inner_mean)


def head_grads(
    query_in, key_input, value_input, grad_in, query_gain, key_gain, cos_tab, sin_tab, block_rows
):
    token_length, groups, per_group, head_dim = query_in.shape
    cos_four = cos_tab[:, None, None, :]
    sin_four = sin_tab[:, None, None, :]
    cos_three = cos_tab[:, None, :]
    sin_three = sin_tab[:, None, :]
    query_f = query_in.astype(jnp.float32)
    query_inv = inverse_rms(query_f)
    query_rot = rotate(query_f * query_inv * query_gain, cos_four, sin_four).astype(jnp.bfloat16)
    key_f = key_input.astype(jnp.float32)
    key_inv = inverse_rms(key_f)
    key_rot = rotate(key_f * key_inv * key_gain, cos_three, sin_three).astype(jnp.bfloat16)
    num_blocks = token_length // block_rows
    query_blocks = query_rot.reshape(num_blocks, block_rows, groups, per_group, head_dim)
    grad_blocks = grad_in.reshape(num_blocks, block_rows, groups, per_group, head_dim)

    def attend_block(carried, pieces):
        key_acc, value_acc = carried
        query_piece, grad_piece = pieces
        scores = product("qgrd,cgd->grqc", query_piece, key_rot) * score_scale
        row_max = jnp.max(scores, axis=-1, keepdims=True)
        shifted = jnp.exp(scores - row_max)
        attn_prob = shifted / jnp.sum(shifted, axis=-1, keepdims=True)
        prob_low = attn_prob.astype(jnp.bfloat16)
        prob_grad = product("qgrd,cgd->grqc", grad_piece, value_input)
        row_dot = jnp.sum(attn_prob * prob_grad, axis=-1, keepdims=True)
        score_grad = (attn_prob * (prob_grad - row_dot) * score_scale).astype(jnp.bfloat16)
        dq_piece = product("grqc,cgd->qgrd", score_grad, key_rot)
        key_acc = key_acc + product("grqc,qgrd->cgd", score_grad, query_piece)
        value_acc = value_acc + product("grqc,qgrd->cgd", prob_low, grad_piece)
        return ((key_acc, value_acc), dq_piece)

    empty_acc = jnp.zeros((token_length, groups, head_dim), jnp.float32)
    (key_rot_grad, value_acc), query_rot_grad = lax.scan(
        attend_block, (empty_acc, empty_acc), (query_blocks, grad_blocks)
    )
    query_rot_grad = query_rot_grad.reshape(token_length, groups, per_group, head_dim)
    query_grad = norm_back(
        query_f, query_inv, rotate_back(query_rot_grad, cos_four, sin_four), query_gain
    ).astype(jnp.bfloat16)
    key_portion = norm_back(
        key_f, key_inv, rotate_back(key_rot_grad, cos_three, sin_three), key_gain
    ).astype(jnp.bfloat16)
    return (query_grad, key_portion, value_acc.astype(jnp.bfloat16))


def generic_device(
    inputs, queries, keys, values, out_grad, query_gain, key_gain, key_matrix, value_matrix
):
    sp_count = lax.axis_size("sp")
    dp_count = lax.axis_size("dp")
    token_row_block = inputs.shape[1]
    token_length = token_row_block * sp_count
    local_heads = QUERY_HEADS // sp_count
    portion_heads = min(local_heads, QUERY_HEADS // KEY_VALUE_HEADS)
    kv_here = local_heads // portion_heads
    group_copies = QUERY_HEADS // KEY_VALUE_HEADS // portion_heads
    key_value_width = KEY_VALUE_HEADS * HEAD_CHANNELS
    key_positions = jnp.repeat(
        keys[0].reshape(token_row_block, KEY_VALUE_HEADS, HEAD_CHANNELS), group_copies, axis=1
    ).reshape(token_row_block, key_value_width * group_copies)
    value_positions = jnp.repeat(
        values[0].reshape(token_row_block, KEY_VALUE_HEADS, HEAD_CHANNELS), group_copies, axis=1
    ).reshape(token_row_block, key_value_width * group_copies)
    grad_heads, query_heads, key_heads, value_heads = (
        lax.all_to_all(out_grad[0], "sp", split_axis=1, concat_axis=0, tiled=True),
        lax.all_to_all(queries[0], "sp", split_axis=1, concat_axis=0, tiled=True),
        lax.all_to_all(key_positions, "sp", split_axis=1, concat_axis=0, tiled=True),
        lax.all_to_all(value_positions, "sp", split_axis=1, concat_axis=0, tiled=True),
    )
    cos_tab, sin_tab = rotary_tables(token_length)
    query_part, key_portion, value_portion = head_grads(
        query_heads.reshape(token_length, kv_here, portion_heads, HEAD_CHANNELS),
        key_heads.reshape(token_length, kv_here, HEAD_CHANNELS),
        value_heads.reshape(token_length, kv_here, HEAD_CHANNELS),
        grad_heads.reshape(token_length, kv_here, portion_heads, HEAD_CHANNELS),
        query_gain,
        key_gain,
        cos_tab,
        sin_tab,
        min(512, token_length),
    )
    query_tokens, key_token_rows, value_token_rows = (
        lax.all_to_all(
            query_part.reshape(token_length, local_heads * HEAD_CHANNELS),
            "sp",
            split_axis=0,
            concat_axis=1,
            tiled=True,
        ),
        lax.all_to_all(
            key_portion.reshape(token_length, kv_here * HEAD_CHANNELS),
            "sp",
            split_axis=0,
            concat_axis=1,
            tiled=True,
        ),
        lax.all_to_all(
            value_portion.reshape(token_length, kv_here * HEAD_CHANNELS),
            "sp",
            split_axis=0,
            concat_axis=1,
            tiled=True,
        ),
    )
    key_gradient = (
        key_token_rows.reshape(token_row_block, KEY_VALUE_HEADS, group_copies, HEAD_CHANNELS)
        .astype(jnp.float32)
        .sum(axis=2)
        .astype(jnp.bfloat16)
    )
    value_gradient = (
        value_token_rows.reshape(token_row_block, KEY_VALUE_HEADS, group_copies, HEAD_CHANNELS)
        .astype(jnp.float32)
        .sum(axis=2)
        .astype(jnp.bfloat16)
    )
    projection_gradient = jnp.concatenate(
        [
            key_gradient.reshape(token_row_block, key_value_width),
            value_gradient.reshape(token_row_block, key_value_width),
        ],
        axis=1,
    )
    joined_weight = jnp.concatenate([key_matrix, value_matrix], axis=1)
    input_grad = lax.dot_general(
        projection_gradient,
        lax.all_gather(joined_weight, "dp", axis=0, tiled=True),
        (((1,), (1,)), ((), ())),
        preferred_element_type=jnp.float32,
    ).astype(jnp.bfloat16)
    token_in = inputs[0]
    width = inputs.shape[2]
    row_share = width // (sp_count * dp_count)
    permuted = (
        token_in.reshape(token_row_block, dp_count, sp_count, row_share)
        .transpose(0, 2, 1, 3)
        .reshape(token_row_block, width)
    )
    share_cols = lax.all_to_all(permuted, "sp", split_axis=1, concat_axis=0, tiled=True)
    all_grads = lax.all_gather(projection_gradient, "sp", axis=0, tiled=True)
    grad_piece = lax.psum_scatter(
        lax.dot_general(
            share_cols, all_grads, (((0,), (0,)), ((), ())), preferred_element_type=jnp.float32
        ).astype(jnp.bfloat16),
        "dp",
        scatter_dimension=0,
        tiled=True,
    ).astype(jnp.float32)
    weight_grad = lax.all_gather(grad_piece, "sp", axis=0, tiled=True)
    return (
        input_grad[None],
        query_tokens[None],
        weight_grad[:, :key_value_width],
        weight_grad[:, key_value_width:],
    )


bf16 = jnp.bfloat16
f32 = jnp.float32


def dot(first_op, second_op, first_dim, second_dim):
    return lax.dot_general(
        first_op, second_op, (((first_dim,), (second_dim,)), ((), ())), preferred_element_type=f32
    )


def kernel_call(body, out_shape, scratch, args, flops=0):
    vmem = pl.BlockSpec(memory_space=pltpu.VMEM)
    return pl.pallas_call(
        body,
        out_shape=out_shape,
        in_specs=[vmem] * len(args),
        out_specs=jax.tree.map(lambda _: vmem, out_shape),
        scratch_shapes=scratch,
        cost_estimate=pl.CostEstimate(flops=flops, bytes_accessed=0, transcendentals=0),
        compiler_params=pltpu.CompilerParams(vmem_limit_bytes=58 * 1024 * 1024),
    )(*args)


def shape_of(shape, dtype=bf16):
    return jax.ShapeDtypeStruct(shape, dtype)


def swap_with(value, axis, k):
    count = lax.axis_size(axis)
    return lax.ppermute(value, axis, [(i, i ^ k) for i in range(count)])


def copy_call(body, out_shape, count, args):
    anywhere = pl.BlockSpec(memory_space=pl.ANY)
    vmem = pl.BlockSpec(memory_space=pltpu.VMEM)

    def run(*refs):
        sems = refs[-1]
        copies = [
            pltpu.make_async_copy(source, target, sems.at[i])
            for i, (source, target) in enumerate(body(*refs[:-1]))
        ]
        for copy in copies:
            copy.start()
        for copy in copies:
            copy.wait()

    return pl.pallas_call(
        run,
        out_shape=out_shape,
        in_specs=[anywhere] * len(args),
        out_specs=jax.tree.map(lambda _: vmem, out_shape),
        scratch_shapes=[pltpu.SemaphoreType.DMA((count,))],
    )(*args)


def lanes_of(half, width):
    return pl.ds(pl.multiple_of(half * width, 128), width)


def pack_heads(queries, keys, values, out_grad):
    rows, q_all = queries.shape
    q_half, kv_half = q_all // 2, keys.shape[1] // 2
    width = 2 * q_half + 2 * kv_half

    def body(q_ref, g_ref, k_ref, v_ref, mate, far, far_mate):
        bit = lax.axis_index("sp") % 2
        pairs = [
            (q_ref.at[:, lanes_of(1 - bit, q_half)], mate.at[:, :q_half]),
            (g_ref.at[:, lanes_of(1 - bit, q_half)], mate.at[:, q_half : 2 * q_half]),
        ]
        for out, half, lo in ((mate, 1 - bit, 2 * q_half), (far, bit, 0), (far_mate, 1 - bit, 0)):
            lanes = lanes_of(half, kv_half)
            pairs.append((k_ref.at[:, lanes], out.at[:, lo : lo + kv_half]))
            pairs.append((v_ref.at[:, lanes], out.at[:, lo + kv_half : lo + 2 * kv_half]))
        return pairs

    return copy_call(
        body,
        [shape_of((rows, width))] + [shape_of((rows, 2 * kv_half))] * 2,
        8,
        (queries, out_grad, keys, values),
    )


def join_weights(key_matrix, value_matrix):
    rows, kv_width = key_matrix.shape
    half = kv_width // 2

    def body(wk_ref, wv_ref, out):
        pairs = []
        for d in range(2):
            cols = slice(d * half, (d + 1) * half)
            pairs.append((wk_ref.at[:, cols], out.at[:, 2 * d * half : (2 * d + 1) * half]))
            pairs.append((wv_ref.at[:, cols], out.at[:, (2 * d + 1) * half : (2 * d + 2) * half]))
        return pairs

    return copy_call(body, shape_of((rows, 2 * kv_width)), 4, (key_matrix, value_matrix))


def turn_inputs(own, mate):
    rows, width = own.shape

    def body(own_ref, mate_ref, out):
        out[:, :rows] = own_ref[...].T
        out[:, rows:] = mate_ref[...].T

    return kernel_call(body, shape_of((width, 2 * rows)), [], (own, mate))


def angle_tables(token_length):
    half_pairs = HEAD_CHANNELS // 4
    inv_freq = rope_base ** (-np.arange(half_pairs, dtype=np.float64) / half_pairs)
    inv_freq = inv_freq.astype(np.float32)
    channel = np.arange(2 * HEAD_CHANNELS)
    freq = inv_freq[(channel % HEAD_CHANNELS // 2) % half_pairs]
    sign = np.where(channel % 2 == 0, -1.0, 1.0).astype(np.float32)
    tables = []
    for count in (token_length // GRID, GRID):
        angles = (np.arange(count, dtype=np.float32)[:, None] * freq).astype(np.float64)
        tables += [np.cos(angles).astype(np.float32), (np.sin(angles) * sign).astype(np.float32)]
    return tables


def attention(queries, out_grad, keys, values, mate, far, far_mate, query_gain, key_gain):
    rows = queries.shape[0]
    q_width = queries.shape[1] // 2
    k_width = keys.shape[1] // 2
    pair = 2 * HEAD_CHANNELS
    heads = q_width // HEAD_CHANNELS
    groups = k_width // HEAD_CHANNELS
    per_group = heads // groups
    half = 2 * rows
    tokens = 4 * rows
    tables = angle_tables(tokens)

    def body(*refs):
        q_ref, g_ref, k_ref, v_ref, mate_ref, far_ref, far_mate_ref = refs[:7]
        qg_ref, kg_ref, row_cos, row_sin, col_cos, col_sin = refs[7:13]
        dq_own, dq_mate, p_own, p_far = refs[13:17]
        q_tok, kv_tok, qh, gh, kr, vv, q_inv, k_inv, dq_sc, dk_sc, dq_out, p_sc, sems = refs[17:]
        me = lax.axis_index("sp")
        bit = me % 2
        upper = me // 2
        q_own = pl.multiple_of(bit * rows, rows)
        q_mate = pl.multiple_of((1 - bit) * rows, rows)

        def kv_rows(k):
            return pl.ds(pl.multiple_of((me ^ k) * rows, rows), rows)

        pairs = [
            (far_ref, kv_tok.at[kv_rows(2), :]),
            (far_mate_ref, kv_tok.at[kv_rows(3), :]),
            (mate_ref.at[:, 2 * q_width :], kv_tok.at[kv_rows(1), :]),
            (k_ref.at[:, lanes_of(bit, k_width)], kv_tok.at[kv_rows(0), :k_width]),
            (v_ref.at[:, lanes_of(bit, k_width)], kv_tok.at[kv_rows(0), k_width:]),
            (q_ref.at[:, lanes_of(bit, q_width)], q_tok.at[pl.ds(q_own, rows), :q_width]),
            (g_ref.at[:, lanes_of(bit, q_width)], q_tok.at[pl.ds(q_own, rows), q_width:]),
            (mate_ref.at[:, : 2 * q_width], q_tok.at[pl.ds(q_mate, rows), :]),
        ]
        copies = [
            pltpu.make_async_copy(source, target, sems.at[i])
            for i, (source, target) in enumerate(pairs)
        ]
        for copy in copies:
            copy.start()
        lane = lax.broadcasted_iota(jnp.int32, (GRID, pair), 1)
        even = lane % 2 == 0
        by_row = lane % HEAD_CHANNELS < HEAD_CHANNELS // 2
        seg_r = lax.broadcasted_iota(jnp.int32, (2 * pair, pair), 0) // HEAD_CHANNELS % 2
        seg_c = lax.broadcasted_iota(jnp.int32, (2 * pair, pair), 1) // HEAD_CHANNELS
        seg = jnp.where(seg_r == seg_c, 1.0 / HEAD_CHANNELS, 0.0).astype(bf16)
        q_gain = jnp.concatenate([qg_ref[...], qg_ref[...]], axis=1)
        k_gain = jnp.concatenate([kg_ref[...], kg_ref[...]], axis=1)

        def head_mean(product_f):
            high = product_f.astype(bf16)
            low = (product_f - high.astype(f32)).astype(bf16)
            return dot(jnp.concatenate([high, low], axis=1), seg, 1, 0)

        def swap(value):
            return jnp.where(even, pltpu.roll(value, pair - 1, 1), pltpu.roll(value, 1, 1))

        def angles_of(r):
            cos = jnp.where(by_row, row_cos[pl.ds(r, 1), :], col_cos[...])
            sin = jnp.where(by_row, row_sin[pl.ds(r, 1), :], col_sin[...])
            return cos, sin

        def forward(value, gain, cos, sin):
            inv = lax.rsqrt(head_mean(value * value) + norm_eps)
            normed = value * inv * gain
            return inv, (normed * cos + swap(normed) * sin).astype(bf16)

        def backward(value, inv, grad, gain, cos, sin):
            weighted = (grad * cos - swap(grad) * sin) * gain
            inner = head_mean(weighted * value)
            return inv * (weighted - value * inv * inv * inner)

        q_rows = half // GRID
        for copy in copies:
            copy.wait()
        for r in range(tokens // GRID):
            at = slice(r * GRID, (r + 1) * GRID)
            cos, sin = angles_of(r)
            for lo in range(0, k_width, pair):
                part = slice(lo, lo + pair)
                inv, turned = forward(kv_tok[at, part].astype(f32), k_gain, cos, sin)
                k_inv[at, part] = inv
                for u in range(2):
                    g = lo // HEAD_CHANNELS + u
                    kr[g, at, :] = turned[:, u * HEAD_CHANNELS : (u + 1) * HEAD_CHANNELS]
                    begin = k_width + g * HEAD_CHANNELS
                    vv[g, at, :] = kv_tok[at, begin : begin + HEAD_CHANNELS]
        for r in range(q_rows):
            at = slice(r * GRID, (r + 1) * GRID)
            cos, sin = angles_of(upper * q_rows + r)
            for lo in range(0, q_width, pair):
                part = slice(lo, lo + pair)
                inv, turned = forward(q_tok[at, part].astype(f32), q_gain, cos, sin)
                q_inv[at, part] = inv
                grad = q_tok[at, q_width + lo : q_width + lo + pair]
                for u in range(2):
                    lanes = slice(u * HEAD_CHANNELS, (u + 1) * HEAD_CHANNELS)
                    qh[lo // HEAD_CHANNELS + u, at, :] = turned[:, lanes]
                    gh[lo // HEAD_CHANNELS + u, at, :] = grad[:, lanes]

        for g in range(groups):
            key_rot = kr[g]
            value_in = vv[g]
            for h in range(g * per_group, (g + 1) * per_group):
                query = qh[h]
                grad = gh[h]
                scores = dot(key_rot, query, 1, 1)
                top = jnp.max(scores, axis=0, keepdims=True)
                expo = jnp.exp((scores - top) * score_scale)
                prob = expo * (1.0 / jnp.sum(expo, axis=0, keepdims=True))
                prob_grad = dot(value_in, grad, 1, 1)
                row_dot = jnp.sum(prob * prob_grad, axis=0, keepdims=True)
                score_grad = (prob * (prob_grad - row_dot)).astype(bf16)
                dv = dot(prob.astype(bf16), grad, 1, 0)
                dk = dot(score_grad, query, 1, 0)
                dq_t = dot(key_rot, score_grad, 0, 0)
                dq_sc[:, h * HEAD_CHANNELS : (h + 1) * HEAD_CHANNELS] = dq_t.T * score_scale
                first = h == g * per_group
                key_acc = dk if first else key_acc + dk
                value_acc = dv if first else value_acc + dv
            lo = g * HEAD_CHANNELS
            dk_sc[:, lo : lo + HEAD_CHANNELS] = key_acc * score_scale
            p_sc[:, k_width + lo : k_width + lo + HEAD_CHANNELS] = value_acc

        for r in range(tokens // GRID):
            at = slice(r * GRID, (r + 1) * GRID)
            cos, sin = angles_of(r)
            for lo in range(0, k_width, pair):
                part = slice(lo, lo + pair)
                value = kv_tok[at, part].astype(f32)
                p_sc[at, part] = backward(value, k_inv[at, part], dk_sc[at, part], k_gain, cos, sin)
        p_own[...] = p_sc[pl.ds(pl.multiple_of(upper * half, half), half), :]
        p_far[...] = p_sc[pl.ds(pl.multiple_of((1 - upper) * half, half), half), :].astype(bf16)
        for r in range(q_rows):
            at = slice(r * GRID, (r + 1) * GRID)
            cos, sin = angles_of(upper * q_rows + r)
            for lo in range(0, q_width, pair):
                part = slice(lo, lo + pair)
                value = q_tok[at, part].astype(f32)
                result = backward(value, q_inv[at, part], dq_sc[at, part], q_gain, cos, sin)
                dq_out[at, part] = result.astype(bf16)
        dq_own[...] = dq_out[pl.ds(q_own, rows), :]
        dq_mate[...] = dq_out[pl.ds(q_mate, rows), :]

    vmem = pl.BlockSpec(memory_space=pltpu.VMEM)
    args = (queries, out_grad, keys, values, mate, far, far_mate)
    small = (query_gain[None], key_gain[None], *[jnp.asarray(t) for t in tables])
    return pl.pallas_call(
        body,
        out_shape=[shape_of((rows, q_width))] * 2
        + [shape_of((half, 2 * k_width), f32), shape_of((half, 2 * k_width))],
        in_specs=[pl.BlockSpec(memory_space=pl.ANY)] * len(args) + [vmem] * len(small),
        out_specs=[vmem] * 4,
        scratch_shapes=[
            pltpu.VMEM((half, 2 * q_width), bf16),
            pltpu.VMEM((tokens, 2 * k_width), bf16),
            pltpu.VMEM((heads, half, HEAD_CHANNELS), bf16),
            pltpu.VMEM((heads, half, HEAD_CHANNELS), bf16),
            pltpu.VMEM((groups, tokens, HEAD_CHANNELS), bf16),
            pltpu.VMEM((groups, tokens, HEAD_CHANNELS), bf16),
            pltpu.VMEM((half, q_width), f32),
            pltpu.VMEM((tokens, k_width), f32),
            pltpu.VMEM((half, q_width), f32),
            pltpu.VMEM((tokens, k_width), f32),
            pltpu.VMEM((half, q_width), bf16),
            pltpu.VMEM((tokens, 2 * k_width), f32),
            pltpu.SemaphoreType.DMA((8,)),
        ],
        cost_estimate=pl.CostEstimate(
            flops=10 * heads * half * tokens * HEAD_CHANNELS, bytes_accessed=0, transcendentals=0
        ),
        compiler_params=pltpu.CompilerParams(vmem_limit_bytes=58 * 1024 * 1024),
        name="attention",
    )(*args, *small)


def weight_partials(turned, p_own, p_far, dp_count):
    feats, half = turned.shape
    rows, cols = half // 2, p_own.shape[1]
    share = feats // dp_count
    chips = dp_count // 2

    def body(x_ref, po_ref, pf_ref, mine_out, mate_out, own_out, send_out, p_sc):
        bit = lax.axis_index("sp") % 2
        mine = lax.axis_index("dp")
        p_sc[...] = (po_ref[...] + pf_ref[...].astype(f32)).astype(bf16)
        p_mine = p_sc[pl.ds(pl.multiple_of(bit * rows, rows), rows), :]
        p_mate = p_sc[pl.ds(pl.multiple_of((1 - bit) * rows, rows), rows), :]
        mine_out[...] = p_mine
        mate_out[...] = p_mate
        p_all = jnp.concatenate([p_mine, p_mate], axis=0)
        for out, flip in ((send_out, 1), (own_out, 0)):
            for m in range(chips):
                start = pl.multiple_of((mine ^ (2 * m + flip)) * share, share)
                out[m] = dot(x_ref[pl.ds(start, share), :], p_all, 1, 0).astype(bf16)

    return kernel_call(
        body,
        [shape_of((rows, cols))] * 2 + [shape_of((chips, share, cols))] * 2,
        [pltpu.VMEM((half, cols), bf16)],
        (turned, p_own, p_far),
        flops=2 * feats * half * cols,
    )


def sum_over_devices(own, sent):
    received = swap_with(sent, "dp", 1)
    chips = own.shape[0]
    paired = [own[m].astype(f32) + received[m].astype(f32) for m in range(chips)]
    total = paired[0]
    for m in range(1, chips):
        total = total + swap_with(paired[m].astype(bf16), "dp", 2 * m).astype(f32)
    return total.astype(bf16)


def join_weight_grads(own, mate, far, far_mate):
    half = own.shape[1] // 2
    here = own.astype(f32) + far.astype(f32)
    there = mate.astype(f32) + far_mate.astype(f32)
    even = lax.axis_index("sp") % 2 == 0
    first = jnp.where(even, here, there)
    second = jnp.where(even, there, here)
    return (
        jnp.concatenate([first[:, :half], second[:, :half]], axis=1),
        jnp.concatenate([first[:, half:], second[:, half:]], axis=1),
    )


def token_outputs(p_mine, p_from_mate, weight_pieces, dq_own, dq_from_mate):
    rows, cols = p_mine.shape
    q_half = dq_own.shape[1]
    dp_count = len(weight_pieces)
    w_rows = weight_pieces[0].shape[0]

    def body(p_ref, pm_ref, dq_ref, dqm_ref, *rest):
        w_refs = rest[:dp_count]
        x_out, q_out, p_buf, out_buf, q_buf = rest[dp_count:]
        bit = lax.axis_index("sp") % 2
        mine = lax.axis_index("dp")
        p_buf[bit] = p_ref[...]
        p_buf[1 - bit] = pm_ref[...]
        q_buf[bit] = dq_ref[...]
        q_buf[1 - bit] = dqm_ref[...]
        for d in range(2):
            q_out[:, d * q_half : (d + 1) * q_half] = q_buf[d]
        left = jnp.concatenate([p_buf[0], p_buf[1]], axis=1)
        for m in range(dp_count):
            out_buf[mine ^ m] = dot(left, w_refs[m][...], 1, 1).astype(bf16)
        for j in range(dp_count):
            x_out[:, j * w_rows : (j + 1) * w_rows] = out_buf[j]

    return kernel_call(
        body,
        [shape_of((rows, dp_count * w_rows)), shape_of((rows, 2 * q_half))],
        [
            pltpu.VMEM((2, rows, cols), bf16),
            pltpu.VMEM((dp_count, rows, w_rows), bf16),
            pltpu.VMEM((2, rows, q_half), bf16),
        ],
        (p_mine, p_from_mate, dq_own, dq_from_mate, *weight_pieces),
        flops=4 * rows * dp_count * w_rows * cols,
    )


def fast_device(
    inputs, queries, keys, values, out_grad, query_gain, key_gain, key_matrix, value_matrix
):
    return fast_body(
        inputs[0],
        queries[0],
        keys[0],
        values[0],
        out_grad[0],
        query_gain,
        key_gain,
        key_matrix,
        value_matrix,
    )


def fast_body(
    inputs, queries, keys, values, out_grad, query_gain, key_gain, key_matrix, value_matrix
):
    dp_count = lax.axis_size("dp")
    mate, far, far_mate = pack_heads(queries, keys, values, out_grad)
    mate = swap_with(mate, "sp", 1)
    far = swap_with(far, "sp", 2)
    far_mate = swap_with(far_mate, "sp", 3)
    joined_weight = join_weights(key_matrix, value_matrix)
    weight_pieces = [joined_weight] + [
        swap_with(joined_weight, "dp", m) for m in range(1, dp_count)
    ]
    mate_inputs = swap_with(inputs, "sp", 1)
    dq_own, dq_mate, p_own, p_far = attention(
        queries, out_grad, keys, values, mate, far, far_mate, query_gain, key_gain
    )
    p_far = swap_with(p_far, "sp", 2)
    dq_mate = swap_with(dq_mate, "sp", 1)
    turned = turn_inputs(inputs, mate_inputs)
    p_mine, p_mate, own, sent = weight_partials(turned, p_own, p_far, dp_count)
    summed = sum_over_devices(own, sent)
    p_mate = swap_with(p_mate, "sp", 1)
    input_grad, query_grad = token_outputs(p_mine, p_mate, weight_pieces, dq_own, dq_mate)
    key_weight, value_weight = join_weight_grads(
        summed, *[swap_with(summed, "sp", k) for k in range(1, 4)]
    )
    return input_grad[None], query_grad[None], key_weight, value_weight


def solution(mesh):
    sp_count, dp_count = mesh.shape["sp"], mesh.shape["dp"]
    fast = sp_count == 4 and dp_count & (dp_count - 1) == 0
    return jax.shard_map(
        fast_device if fast else generic_device,
        mesh=mesh,
        in_specs=(
            P("dp", "sp", None),
            P("dp", "sp", None),
            P("dp", "sp", None),
            P("dp", "sp", None),
            P("dp", "sp", None),
            P(),
            P(),
            P("dp", None),
            P("dp", None),
        ),
        out_specs=(P("dp", "sp", None), P("dp", "sp", None), P("dp", None), P("dp", None)),
        check_vma=False,
    )
```

```python
import jax
import jax.numpy as jnp
import numpy as np
from jax import lax
from jax.experimental import pallas as pl
from jax.experimental.pallas import tpu as pltpu
from jax.sharding import PartitionSpec as P

QUERY_HEADS = 16
KEY_VALUE_HEADS = 4
HEAD_CHANNELS = 64
GRID = 64


rope_base = 10000.0
norm_eps = 0.5
score_scale = 0.125


def product(pattern, first_op, second_op):
    return jnp.einsum(pattern, first_op, second_op, preferred_element_type=jnp.float32)


def rotary_tables(token_length):
    position = jnp.arange(token_length, dtype=jnp.int32)
    grid_row = (position // GRID).astype(jnp.float32)
    grid_col = (position % GRID).astype(jnp.float32)
    half_pairs = HEAD_CHANNELS // 4
    inv_freq = rope_base ** (-jnp.arange(half_pairs, dtype=jnp.float32) / half_pairs)
    angles = jnp.concatenate([grid_row[:, None] * inv_freq, grid_col[:, None] * inv_freq], axis=1)
    return (jnp.cos(angles), jnp.sin(angles))


def rotate(vector, cos_tab, sin_tab):
    even_part = vector[..., 0::2]
    odd_part = vector[..., 1::2]
    turned = jnp.stack(
        [even_part * cos_tab - odd_part * sin_tab, even_part * sin_tab + odd_part * cos_tab],
        axis=-1,
    )
    return turned.reshape(vector.shape)


def rotate_back(cotangent, cos_tab, sin_tab):
    even_part = cotangent[..., 0::2]
    odd_part = cotangent[..., 1::2]
    turned = jnp.stack(
        [even_part * cos_tab + odd_part * sin_tab, odd_part * cos_tab - even_part * sin_tab],
        axis=-1,
    )
    return turned.reshape(cotangent.shape)


def inverse_rms(vector):
    return lax.rsqrt(jnp.mean(vector * vector, axis=-1, keepdims=True) + norm_eps)


def norm_back(vector, inv_scale, cotangent, gain_vec):
    weighted = cotangent * gain_vec
    inner_mean = jnp.mean(weighted * vector, axis=-1, keepdims=True)
    return inv_scale * (weighted - vector * inv_scale * inv_scale * inner_mean)


def head_grads(
    query_in, key_input, value_input, grad_in, query_gain, key_gain, cos_tab, sin_tab, block_rows
):
    token_length, groups, per_group, head_dim = query_in.shape
    cos_four = cos_tab[:, None, None, :]
    sin_four = sin_tab[:, None, None, :]
    cos_three = cos_tab[:, None, :]
    sin_three = sin_tab[:, None, :]
    query_f = query_in.astype(jnp.float32)
    query_inv = inverse_rms(query_f)
    query_rot = rotate(query_f * query_inv * query_gain, cos_four, sin_four).astype(jnp.bfloat16)
    key_f = key_input.astype(jnp.float32)
    key_inv = inverse_rms(key_f)
    key_rot = rotate(key_f * key_inv * key_gain, cos_three, sin_three).astype(jnp.bfloat16)
    num_blocks = token_length // block_rows
    query_blocks = query_rot.reshape(num_blocks, block_rows, groups, per_group, head_dim)
    grad_blocks = grad_in.reshape(num_blocks, block_rows, groups, per_group, head_dim)

    def attend_block(carried, pieces):
        key_acc, value_acc = carried
        query_piece, grad_piece = pieces
        scores = product("qgrd,cgd->grqc", query_piece, key_rot) * score_scale
        row_max = jnp.max(scores, axis=-1, keepdims=True)
        shifted = jnp.exp(scores - row_max)
        attn_prob = shifted / jnp.sum(shifted, axis=-1, keepdims=True)
        prob_low = attn_prob.astype(jnp.bfloat16)
        prob_grad = product("qgrd,cgd->grqc", grad_piece, value_input)
        row_dot = jnp.sum(attn_prob * prob_grad, axis=-1, keepdims=True)
        score_grad = (attn_prob * (prob_grad - row_dot) * score_scale).astype(jnp.bfloat16)
        dq_piece = product("grqc,cgd->qgrd", score_grad, key_rot)
        key_acc = key_acc + product("grqc,qgrd->cgd", score_grad, query_piece)
        value_acc = value_acc + product("grqc,qgrd->cgd", prob_low, grad_piece)
        return ((key_acc, value_acc), dq_piece)

    empty_acc = jnp.zeros((token_length, groups, head_dim), jnp.float32)
    (key_rot_grad, value_acc), query_rot_grad = lax.scan(
        attend_block, (empty_acc, empty_acc), (query_blocks, grad_blocks)
    )
    query_rot_grad = query_rot_grad.reshape(token_length, groups, per_group, head_dim)
    query_grad = norm_back(
        query_f, query_inv, rotate_back(query_rot_grad, cos_four, sin_four), query_gain
    ).astype(jnp.bfloat16)
    key_portion = norm_back(
        key_f, key_inv, rotate_back(key_rot_grad, cos_three, sin_three), key_gain
    ).astype(jnp.bfloat16)
    return (query_grad, key_portion, value_acc.astype(jnp.bfloat16))


def generic_device(
    inputs, queries, keys, values, out_grad, query_gain, key_gain, key_matrix, value_matrix
):
    sp_count = lax.axis_size("sp")
    dp_count = lax.axis_size("dp")
    token_row_block = inputs.shape[1]
    token_length = token_row_block * sp_count
    local_heads = QUERY_HEADS // sp_count
    portion_heads = min(local_heads, QUERY_HEADS // KEY_VALUE_HEADS)
    kv_here = local_heads // portion_heads
    group_copies = QUERY_HEADS // KEY_VALUE_HEADS // portion_heads
    key_value_width = KEY_VALUE_HEADS * HEAD_CHANNELS
    key_positions = jnp.repeat(
        keys[0].reshape(token_row_block, KEY_VALUE_HEADS, HEAD_CHANNELS), group_copies, axis=1
    ).reshape(token_row_block, key_value_width * group_copies)
    value_positions = jnp.repeat(
        values[0].reshape(token_row_block, KEY_VALUE_HEADS, HEAD_CHANNELS), group_copies, axis=1
    ).reshape(token_row_block, key_value_width * group_copies)
    grad_heads, query_heads, key_heads, value_heads = (
        lax.all_to_all(out_grad[0], "sp", split_axis=1, concat_axis=0, tiled=True),
        lax.all_to_all(queries[0], "sp", split_axis=1, concat_axis=0, tiled=True),
        lax.all_to_all(key_positions, "sp", split_axis=1, concat_axis=0, tiled=True),
        lax.all_to_all(value_positions, "sp", split_axis=1, concat_axis=0, tiled=True),
    )
    cos_tab, sin_tab = rotary_tables(token_length)
    query_part, key_portion, value_portion = head_grads(
        query_heads.reshape(token_length, kv_here, portion_heads, HEAD_CHANNELS),
        key_heads.reshape(token_length, kv_here, HEAD_CHANNELS),
        value_heads.reshape(token_length, kv_here, HEAD_CHANNELS),
        grad_heads.reshape(token_length, kv_here, portion_heads, HEAD_CHANNELS),
        query_gain,
        key_gain,
        cos_tab,
        sin_tab,
        min(512, token_length),
    )
    query_tokens, key_token_rows, value_token_rows = (
        lax.all_to_all(
            query_part.reshape(token_length, local_heads * HEAD_CHANNELS),
            "sp",
            split_axis=0,
            concat_axis=1,
            tiled=True,
        ),
        lax.all_to_all(
            key_portion.reshape(token_length, kv_here * HEAD_CHANNELS),
            "sp",
            split_axis=0,
            concat_axis=1,
            tiled=True,
        ),
        lax.all_to_all(
            value_portion.reshape(token_length, kv_here * HEAD_CHANNELS),
            "sp",
            split_axis=0,
            concat_axis=1,
            tiled=True,
        ),
    )
    key_gradient = (
        key_token_rows.reshape(token_row_block, KEY_VALUE_HEADS, group_copies, HEAD_CHANNELS)
        .astype(jnp.float32)
        .sum(axis=2)
        .astype(jnp.bfloat16)
    )
    value_gradient = (
        value_token_rows.reshape(token_row_block, KEY_VALUE_HEADS, group_copies, HEAD_CHANNELS)
        .astype(jnp.float32)
        .sum(axis=2)
        .astype(jnp.bfloat16)
    )
    projection_gradient = jnp.concatenate(
        [
            key_gradient.reshape(token_row_block, key_value_width),
            value_gradient.reshape(token_row_block, key_value_width),
        ],
        axis=1,
    )
    joined_weight = jnp.concatenate([key_matrix, value_matrix], axis=1)
    input_grad = lax.dot_general(
        projection_gradient,
        lax.all_gather(joined_weight, "dp", axis=0, tiled=True),
        (((1,), (1,)), ((), ())),
        preferred_element_type=jnp.float32,
    ).astype(jnp.bfloat16)
    token_in = inputs[0]
    width = inputs.shape[2]
    row_share = width // (sp_count * dp_count)
    permuted = (
        token_in.reshape(token_row_block, dp_count, sp_count, row_share)
        .transpose(0, 2, 1, 3)
        .reshape(token_row_block, width)
    )
    share_cols = lax.all_to_all(permuted, "sp", split_axis=1, concat_axis=0, tiled=True)
    all_grads = lax.all_gather(projection_gradient, "sp", axis=0, tiled=True)
    grad_piece = lax.psum_scatter(
        lax.dot_general(
            share_cols, all_grads, (((0,), (0,)), ((), ())), preferred_element_type=jnp.float32
        ).astype(jnp.bfloat16),
        "dp",
        scatter_dimension=0,
        tiled=True,
    ).astype(jnp.float32)
    weight_grad = lax.all_gather(grad_piece, "sp", axis=0, tiled=True)
    return (
        input_grad[None],
        query_tokens[None],
        weight_grad[:, :key_value_width],
        weight_grad[:, key_value_width:],
    )


bf16 = jnp.bfloat16
f32 = jnp.float32


def dot(first_op, second_op, first_dim, second_dim):
    return lax.dot_general(
        first_op, second_op, (((first_dim,), (second_dim,)), ((), ())), preferred_element_type=f32
    )


MIB = 1024 * 1024


def in_vmem(value):
    return pltpu.with_memory_space_constraint(value, pltpu.VMEM)


def kernel_call(body, out_shape, scratch, args, flops=0, limit=12 * MIB):
    vmem = pl.BlockSpec(memory_space=pltpu.VMEM)
    return pl.pallas_call(
        body,
        out_shape=out_shape,
        in_specs=[vmem] * len(args),
        out_specs=[vmem] * len(out_shape),
        scratch_shapes=scratch,
        cost_estimate=pl.CostEstimate(flops=flops, bytes_accessed=0, transcendentals=0),
        compiler_params=pltpu.CompilerParams(vmem_limit_bytes=limit),
    )(*[in_vmem(arg) for arg in args])


def held(shape, dtype=bf16):
    return pltpu.VMEM(shape, dtype)


def shape_of(shape, dtype=bf16):
    return jax.ShapeDtypeStruct(shape, dtype)


def swap_with(value, axis, k):
    count = lax.axis_size(axis)
    return lax.ppermute(value, axis, [(i, i ^ k) for i in range(count)])


def copy_call(body, out_shape, count, args):
    def run(*refs):
        sems = refs[-1]
        copies = [
            pltpu.make_async_copy(source, target, sems.at[i])
            for i, (source, target) in enumerate(body(*refs[:-1]))
        ]
        for copy in copies:
            copy.start()
        for copy in copies:
            copy.wait()

    return pl.pallas_call(
        run,
        out_shape=out_shape,
        in_specs=[pl.BlockSpec(memory_space=pltpu.HBM)] * len(args),
        out_specs=[pl.BlockSpec(memory_space=pltpu.VMEM)] * len(out_shape),
        scratch_shapes=[pltpu.SemaphoreType.DMA((count,))],
        compiler_params=pltpu.CompilerParams(vmem_limit_bytes=4 * MIB),
    )(*[pltpu.with_memory_space_constraint(arg, pltpu.HBM) for arg in args])


def lanes_of(half, width):
    return pl.ds(pl.multiple_of(half * width, 128), width)


def head_copies(refs, out, half, q_half, kv_half):
    pairs = []
    lo = 0
    for ref, width in zip(refs, (q_half, q_half, kv_half, kv_half)):
        pairs.append((ref.at[:, lanes_of(half, width)], out.at[:, lo : lo + width]))
        lo += width
    return pairs


def pack_heads(queries, keys, values, out_grad):
    rows, q_all = queries.shape
    q_half, kv_half = q_all // 2, keys.shape[1] // 2

    def body(q_ref, g_ref, k_ref, v_ref, mate, far, far_mate):
        bit = lax.axis_index("sp") % 2
        pairs = head_copies((q_ref, g_ref, k_ref, v_ref), mate, 1 - bit, q_half, kv_half)
        for out, half in ((far, bit), (far_mate, 1 - bit)):
            lanes = lanes_of(half, kv_half)
            pairs.append((k_ref.at[:, lanes], out.at[:, :kv_half]))
            pairs.append((v_ref.at[:, lanes], out.at[:, kv_half:]))
        return pairs

    return copy_call(
        body,
        [held((rows, 2 * q_half + 2 * kv_half))] + [held((rows, 2 * kv_half))] * 2,
        8,
        (queries, out_grad, keys, values),
    )


def pack_own(queries, keys, values, out_grad, key_matrix, value_matrix, query_gain, key_gain):
    rows, q_all = queries.shape
    q_half, kv_half = q_all // 2, keys.shape[1] // 2

    def body(q_ref, g_ref, k_ref, v_ref, wk_ref, wv_ref, qg_ref, kg_ref, own, weight, qg_out, kg_out):
        bit = lax.axis_index("sp") % 2
        pairs = head_copies((q_ref, g_ref, k_ref, v_ref), own, bit, q_half, kv_half)
        for d in range(2):
            cols = slice(d * kv_half, (d + 1) * kv_half)
            for ref, at in ((wk_ref, 2 * d), (wv_ref, 2 * d + 1)):
                pairs.append((ref.at[:, cols], weight.at[:, at * kv_half : (at + 1) * kv_half]))
        return pairs + [(qg_ref, qg_out), (kg_ref, kg_out)]

    return copy_call(
        body,
        [held((rows, 2 * q_half + 2 * kv_half)), held((key_matrix.shape[0], 4 * kv_half))]
        + [held((1, HEAD_CHANNELS), f32)] * 2,
        10,
        (queries, out_grad, keys, values, key_matrix, value_matrix, query_gain[None], key_gain[None]),
    )


def turn_inputs(own, mate):
    rows, width = own.shape

    def body(own_ref, mate_ref, out):
        out[:, :rows] = own_ref[...].T
        out[:, rows:] = mate_ref[...].T

    return kernel_call(body, [held((width, 2 * rows))], [], (own, mate))[0]


def angle_tables(token_length):
    half_pairs = HEAD_CHANNELS // 4
    inv_freq = rope_base ** (-np.arange(half_pairs, dtype=np.float64) / half_pairs)
    inv_freq = inv_freq.astype(np.float32)
    channel = np.arange(2 * HEAD_CHANNELS)
    freq = inv_freq[(channel % HEAD_CHANNELS // 2) % half_pairs]
    sign = np.where(channel % 2 == 0, -1.0, 1.0).astype(np.float32)
    tables = []
    for count in (token_length // GRID, GRID):
        angles = (np.arange(count, dtype=np.float32)[:, None] * freq).astype(np.float64)
        tables += [np.cos(angles).astype(np.float32), (np.sin(angles) * sign).astype(np.float32)]
    return tables


def attention(own, mate, far, far_mate, query_gain, key_gain):
    rows, width = own.shape
    k_width = far.shape[1] // 2
    q_width = width // 2 - k_width
    pair = 2 * HEAD_CHANNELS
    heads = q_width // HEAD_CHANNELS
    groups = k_width // HEAD_CHANNELS
    per_group = heads // groups
    half = 2 * rows
    tokens = 4 * rows
    tables = angle_tables(tokens)

    def body(*refs):
        own_ref, mate_ref, far_ref, far_mate_ref = refs[:4]
        qg_ref, kg_ref, row_cos, row_sin, col_cos, col_sin = refs[4:10]
        dq_own, dq_mate, p_own, p_far = refs[10:14]
        q_tok, kv_tok, qh, gh, kr, vv, q_inv, k_inv, dq_sc, dk_sc, dq_out, p_sc = refs[14:]
        me = lax.axis_index("sp")
        bit = me % 2
        upper = me // 2
        q_own = pl.multiple_of(bit * rows, rows)
        q_mate = pl.multiple_of((1 - bit) * rows, rows)

        q_tok[pl.ds(q_own, rows), :] = own_ref[:, : 2 * q_width]
        q_tok[pl.ds(q_mate, rows), :] = mate_ref[:, : 2 * q_width]
        for k, block in enumerate(
            (own_ref[:, 2 * q_width :], mate_ref[:, 2 * q_width :], far_ref[...], far_mate_ref[...])
        ):
            kv_tok[pl.ds(pl.multiple_of((me ^ k) * rows, rows), rows), :] = block
        lane = lax.broadcasted_iota(jnp.int32, (GRID, pair), 1)
        even = lane % 2 == 0
        by_row = lane % HEAD_CHANNELS < HEAD_CHANNELS // 2
        seg_r = lax.broadcasted_iota(jnp.int32, (2 * pair, pair), 0) // HEAD_CHANNELS % 2
        seg_c = lax.broadcasted_iota(jnp.int32, (2 * pair, pair), 1) // HEAD_CHANNELS
        seg = jnp.where(seg_r == seg_c, 1.0 / HEAD_CHANNELS, 0.0).astype(bf16)
        q_gain = jnp.concatenate([qg_ref[...], qg_ref[...]], axis=1)
        k_gain = jnp.concatenate([kg_ref[...], kg_ref[...]], axis=1)

        def head_mean(product_f):
            high = product_f.astype(bf16)
            low = (product_f - high.astype(f32)).astype(bf16)
            return dot(jnp.concatenate([high, low], axis=1), seg, 1, 0)

        def swap(value):
            return jnp.where(even, pltpu.roll(value, pair - 1, 1), pltpu.roll(value, 1, 1))

        def angles_of(r):
            cos = jnp.where(by_row, row_cos[pl.ds(r, 1), :], col_cos[...])
            sin = jnp.where(by_row, row_sin[pl.ds(r, 1), :], col_sin[...])
            return cos, sin

        def forward(value, gain, cos, sin):
            inv = lax.rsqrt(head_mean(value * value) + norm_eps)
            normed = value * inv * gain
            return inv, (normed * cos + swap(normed) * sin).astype(bf16)

        def backward(value, inv, grad, gain, cos, sin):
            weighted = (grad * cos - swap(grad) * sin) * gain
            inner = head_mean(weighted * value)
            return inv * (weighted - value * inv * inv * inner)

        q_rows = half // GRID
        for r in range(tokens // GRID):
            at = slice(r * GRID, (r + 1) * GRID)
            cos, sin = angles_of(r)
            for lo in range(0, k_width, pair):
                part = slice(lo, lo + pair)
                inv, turned = forward(kv_tok[at, part].astype(f32), k_gain, cos, sin)
                k_inv[at, part] = inv
                for u in range(2):
                    g = lo // HEAD_CHANNELS + u
                    kr[g, at, :] = turned[:, u * HEAD_CHANNELS : (u + 1) * HEAD_CHANNELS]
                    begin = k_width + g * HEAD_CHANNELS
                    vv[g, at, :] = kv_tok[at, begin : begin + HEAD_CHANNELS]
        for r in range(q_rows):
            at = slice(r * GRID, (r + 1) * GRID)
            cos, sin = angles_of(upper * q_rows + r)
            for lo in range(0, q_width, pair):
                part = slice(lo, lo + pair)
                inv, turned = forward(q_tok[at, part].astype(f32), q_gain, cos, sin)
                q_inv[at, part] = inv
                grad = q_tok[at, q_width + lo : q_width + lo + pair]
                for u in range(2):
                    lanes = slice(u * HEAD_CHANNELS, (u + 1) * HEAD_CHANNELS)
                    qh[lo // HEAD_CHANNELS + u, at, :] = turned[:, lanes]
                    gh[lo // HEAD_CHANNELS + u, at, :] = grad[:, lanes]

        for g in range(groups):
            key_rot = kr[g]
            value_in = vv[g]
            for h in range(g * per_group, (g + 1) * per_group):
                query = qh[h]
                grad = gh[h]
                scores = dot(key_rot, query, 1, 1)
                top = jnp.max(scores, axis=0, keepdims=True)
                expo = jnp.exp((scores - top) * score_scale)
                prob = expo * (1.0 / jnp.sum(expo, axis=0, keepdims=True))
                prob_grad = dot(value_in, grad, 1, 1)
                row_dot = jnp.sum(prob * prob_grad, axis=0, keepdims=True)
                score_grad = (prob * (prob_grad - row_dot)).astype(bf16)
                dv = dot(prob.astype(bf16), grad, 1, 0)
                dk = dot(score_grad, query, 1, 0)
                dq_t = dot(key_rot, score_grad, 0, 0)
                dq_sc[:, h * HEAD_CHANNELS : (h + 1) * HEAD_CHANNELS] = dq_t.T * score_scale
                first = h == g * per_group
                key_acc = dk if first else key_acc + dk
                value_acc = dv if first else value_acc + dv
            lo = g * HEAD_CHANNELS
            dk_sc[:, lo : lo + HEAD_CHANNELS] = key_acc * score_scale
            p_sc[:, k_width + lo : k_width + lo + HEAD_CHANNELS] = value_acc

        for r in range(tokens // GRID):
            at = slice(r * GRID, (r + 1) * GRID)
            cos, sin = angles_of(r)
            for lo in range(0, k_width, pair):
                part = slice(lo, lo + pair)
                value = kv_tok[at, part].astype(f32)
                p_sc[at, part] = backward(value, k_inv[at, part], dk_sc[at, part], k_gain, cos, sin)
        p_own[...] = p_sc[pl.ds(pl.multiple_of(upper * half, half), half), :]
        p_far[...] = p_sc[pl.ds(pl.multiple_of((1 - upper) * half, half), half), :].astype(bf16)
        for r in range(q_rows):
            at = slice(r * GRID, (r + 1) * GRID)
            cos, sin = angles_of(upper * q_rows + r)
            for lo in range(0, q_width, pair):
                part = slice(lo, lo + pair)
                value = q_tok[at, part].astype(f32)
                result = backward(value, q_inv[at, part], dq_sc[at, part], q_gain, cos, sin)
                dq_out[at, part] = result.astype(bf16)
        dq_own[...] = dq_out[pl.ds(q_own, rows), :]
        dq_mate[...] = dq_out[pl.ds(q_mate, rows), :]

    return kernel_call(
        body,
        [held((rows, q_width))] * 2 + [held((half, 2 * k_width), f32), held((half, 2 * k_width))],
        [
            pltpu.VMEM((half, 2 * q_width), bf16),
            pltpu.VMEM((tokens, 2 * k_width), bf16),
            pltpu.VMEM((heads, half, HEAD_CHANNELS), bf16),
            pltpu.VMEM((heads, half, HEAD_CHANNELS), bf16),
            pltpu.VMEM((groups, tokens, HEAD_CHANNELS), bf16),
            pltpu.VMEM((groups, tokens, HEAD_CHANNELS), bf16),
            pltpu.VMEM((half, q_width), f32),
            pltpu.VMEM((tokens, k_width), f32),
            pltpu.VMEM((half, q_width), f32),
            pltpu.VMEM((tokens, k_width), f32),
            pltpu.VMEM((half, q_width), bf16),
            pltpu.VMEM((tokens, 2 * k_width), f32),
        ],
        (
            own,
            mate,
            far,
            far_mate,
            query_gain,
            key_gain,
            *[jnp.asarray(table) for table in tables],
        ),
        flops=10 * heads * half * tokens * HEAD_CHANNELS,
        limit=32 * MIB,
    )


def weight_partials(turned, p_own, p_far, dp_count):
    feats, half = turned.shape
    rows, cols = half // 2, p_own.shape[1]
    share = feats // dp_count
    chips = dp_count // 2

    def body(x_ref, po_ref, pf_ref, mine_out, mate_out, own_out, send_out, p_sc):
        bit = lax.axis_index("sp") % 2
        mine = lax.axis_index("dp")
        p_sc[...] = (po_ref[...] + pf_ref[...].astype(f32)).astype(bf16)
        p_mine = p_sc[pl.ds(pl.multiple_of(bit * rows, rows), rows), :]
        p_mate = p_sc[pl.ds(pl.multiple_of((1 - bit) * rows, rows), rows), :]
        mine_out[...] = p_mine
        mate_out[...] = p_mate
        p_all = jnp.concatenate([p_mine, p_mate], axis=0)
        for out, flip in ((send_out, 1), (own_out, 0)):
            for m in range(chips):
                start = pl.multiple_of((mine ^ (2 * m + flip)) * share, share)
                out[m] = dot(x_ref[pl.ds(start, share), :], p_all, 1, 0).astype(bf16)

    return kernel_call(
        body,
        [held((rows, cols))] * 2 + [held((chips, share, cols))] * 2,
        [pltpu.VMEM((half, cols), bf16)],
        (turned, p_own, p_far),
        flops=2 * feats * half * cols,
    )


def sum_over_devices(own, sent):
    received = swap_with(sent, "dp", 1)
    chips = own.shape[0]
    paired = [own[m].astype(f32) + received[m].astype(f32) for m in range(chips)]
    total = paired[0]
    for m in range(1, chips):
        total = total + swap_with(paired[m].astype(bf16), "dp", 2 * m).astype(f32)
    return total.astype(bf16)


def join_weight_grads(own, mate, far, far_mate):
    rows, cols = own.shape
    half = cols // 2

    def body(own_ref, mate_ref, far_ref, far_mate_ref, k_out, v_out, k_sc, v_sc, sems):
        even = lax.axis_index("sp") % 2 == 0
        here = own_ref[...].astype(f32) + far_ref[...].astype(f32)
        there = mate_ref[...].astype(f32) + far_mate_ref[...].astype(f32)
        copies = []
        for i, (scratch, out, lanes) in enumerate(
            ((k_sc, k_out, slice(0, half)), (v_sc, v_out, slice(half, cols)))
        ):
            scratch[:, :half] = jnp.where(even, here[:, lanes], there[:, lanes])
            scratch[:, half:] = jnp.where(even, there[:, lanes], here[:, lanes])
            copy = pltpu.make_async_copy(scratch, out, sems.at[i])
            copy.start()
            copies.append(copy)
        for copy in copies:
            copy.wait()

    return pl.pallas_call(
        body,
        out_shape=[shape_of((rows, cols), f32)] * 2,
        in_specs=[pl.BlockSpec(memory_space=pltpu.VMEM)] * 4,
        out_specs=[pl.BlockSpec(memory_space=pltpu.HBM)] * 2,
        scratch_shapes=[pltpu.VMEM((rows, cols), f32)] * 2 + [pltpu.SemaphoreType.DMA((2,))],
        compiler_params=pltpu.CompilerParams(vmem_limit_bytes=4 * MIB),
        name="join_weight_grads",
    )(*[in_vmem(piece) for piece in (own, mate, far, far_mate)])


def token_outputs(p_mine, p_from_mate, weight_pieces, dq_own, dq_from_mate):
    rows, cols = p_mine.shape
    q_half = dq_own.shape[1]
    dp_count = len(weight_pieces)
    w_rows = weight_pieces[0].shape[0]

    def body(p_ref, pm_ref, dq_ref, dqm_ref, *rest):
        w_refs = rest[:dp_count]
        x_out, q_out, p_buf, out_buf, q_buf = rest[dp_count:]
        bit = lax.axis_index("sp") % 2
        mine = lax.axis_index("dp")
        p_buf[bit] = p_ref[...]
        p_buf[1 - bit] = pm_ref[...]
        q_buf[bit] = dq_ref[...]
        q_buf[1 - bit] = dqm_ref[...]
        for d in range(2):
            q_out[:, d * q_half : (d + 1) * q_half] = q_buf[d]
        left = jnp.concatenate([p_buf[0], p_buf[1]], axis=1)
        for m in range(dp_count):
            out_buf[mine ^ m] = dot(left, w_refs[m][...], 1, 1).astype(bf16)
        for j in range(dp_count):
            x_out[:, j * w_rows : (j + 1) * w_rows] = out_buf[j]

    return kernel_call(
        body,
        [shape_of((rows, dp_count * w_rows)), shape_of((rows, 2 * q_half))],
        [
            pltpu.VMEM((2, rows, cols), bf16),
            pltpu.VMEM((dp_count, rows, w_rows), bf16),
            pltpu.VMEM((2, rows, q_half), bf16),
        ],
        (p_mine, p_from_mate, dq_own, dq_from_mate, *weight_pieces),
        flops=4 * rows * dp_count * w_rows * cols,
    )


def fast_device(
    inputs, queries, keys, values, out_grad, query_gain, key_gain, key_matrix, value_matrix
):
    return fast_body(
        inputs[0],
        queries[0],
        keys[0],
        values[0],
        out_grad[0],
        query_gain,
        key_gain,
        key_matrix,
        value_matrix,
    )


def fast_body(
    inputs, queries, keys, values, out_grad, query_gain, key_gain, key_matrix, value_matrix
):
    dp_count = lax.axis_size("dp")
    mate, far, far_mate = pack_heads(queries, keys, values, out_grad)
    mate = swap_with(mate, "sp", 1)
    far = swap_with(far, "sp", 2)
    far_mate = swap_with(far_mate, "sp", 3)
    own, joined_weight, query_gain, key_gain = pack_own(
        queries, keys, values, out_grad, key_matrix, value_matrix, query_gain, key_gain
    )
    weight_pieces = [joined_weight] + [
        swap_with(joined_weight, "dp", m) for m in range(1, dp_count)
    ]
    mate_inputs = swap_with(inputs, "sp", 1)
    dq_own, dq_mate, p_own, p_far = attention(own, mate, far, far_mate, query_gain, key_gain)
    p_far = swap_with(p_far, "sp", 2)
    dq_mate = swap_with(dq_mate, "sp", 1)
    turned = turn_inputs(inputs, mate_inputs)
    p_mine, p_mate, own, sent = weight_partials(turned, p_own, p_far, dp_count)
    summed = sum_over_devices(own, sent)
    p_mate = swap_with(p_mate, "sp", 1)
    input_grad, query_grad = token_outputs(p_mine, p_mate, weight_pieces, dq_own, dq_mate)
    key_weight, value_weight = join_weight_grads(
        summed, *[swap_with(summed, "sp", k) for k in range(1, 4)]
    )
    return input_grad[None], query_grad[None], key_weight, value_weight


def solution(mesh):
    sp_count, dp_count = mesh.shape["sp"], mesh.shape["dp"]
    fast = sp_count == 4 and dp_count & (dp_count - 1) == 0
    return jax.shard_map(
        fast_device if fast else generic_device,
        mesh=mesh,
        in_specs=(
            P("dp", "sp", None),
            P("dp", "sp", None),
            P("dp", "sp", None),
            P("dp", "sp", None),
            P("dp", "sp", None),
            P(),
            P(),
            P("dp", None),
            P("dp", None),
        ),
        out_specs=(P("dp", "sp", None), P("dp", "sp", None), P("dp", None), P("dp", None)),
        check_vma=False,
    )
```

```python
import jax
import jax.numpy as jnp
import numpy as np
from jax import lax
from jax.experimental import pallas as pl
from jax.experimental.pallas import tpu as pltpu
from jax.sharding import PartitionSpec as P

QUERY_HEADS = 16
KEY_VALUE_HEADS = 4
HEAD_CHANNELS = 64
GRID = 64


rope_base = 10000.0
norm_eps = 0.5
score_scale = 0.125


def product(pattern, first_op, second_op):
    return jnp.einsum(pattern, first_op, second_op, preferred_element_type=jnp.float32)


def rotary_tables(token_length):
    position = jnp.arange(token_length, dtype=jnp.int32)
    grid_row = (position // GRID).astype(jnp.float32)
    grid_col = (position % GRID).astype(jnp.float32)
    half_pairs = HEAD_CHANNELS // 4
    inv_freq = rope_base ** (-jnp.arange(half_pairs, dtype=jnp.float32) / half_pairs)
    angles = jnp.concatenate([grid_row[:, None] * inv_freq, grid_col[:, None] * inv_freq], axis=1)
    return (jnp.cos(angles), jnp.sin(angles))


def rotate(vector, cos_tab, sin_tab):
    even_part = vector[..., 0::2]
    odd_part = vector[..., 1::2]
    turned = jnp.stack(
        [even_part * cos_tab - odd_part * sin_tab, even_part * sin_tab + odd_part * cos_tab],
        axis=-1,
    )
    return turned.reshape(vector.shape)


def rotate_back(cotangent, cos_tab, sin_tab):
    even_part = cotangent[..., 0::2]
    odd_part = cotangent[..., 1::2]
    turned = jnp.stack(
        [even_part * cos_tab + odd_part * sin_tab, odd_part * cos_tab - even_part * sin_tab],
        axis=-1,
    )
    return turned.reshape(cotangent.shape)


def inverse_rms(vector):
    return lax.rsqrt(jnp.mean(vector * vector, axis=-1, keepdims=True) + norm_eps)


def norm_back(vector, inv_scale, cotangent, gain_vec):
    weighted = cotangent * gain_vec
    inner_mean = jnp.mean(weighted * vector, axis=-1, keepdims=True)
    return inv_scale * (weighted - vector * inv_scale * inv_scale * inner_mean)


def head_grads(
    query_in, key_input, value_input, grad_in, query_gain, key_gain, cos_tab, sin_tab, block_rows
):
    token_length, groups, per_group, head_dim = query_in.shape
    cos_four = cos_tab[:, None, None, :]
    sin_four = sin_tab[:, None, None, :]
    cos_three = cos_tab[:, None, :]
    sin_three = sin_tab[:, None, :]
    query_f = query_in.astype(jnp.float32)
    query_inv = inverse_rms(query_f)
    query_rot = rotate(query_f * query_inv * query_gain, cos_four, sin_four).astype(jnp.bfloat16)
    key_f = key_input.astype(jnp.float32)
    key_inv = inverse_rms(key_f)
    key_rot = rotate(key_f * key_inv * key_gain, cos_three, sin_three).astype(jnp.bfloat16)
    num_blocks = token_length // block_rows
    query_blocks = query_rot.reshape(num_blocks, block_rows, groups, per_group, head_dim)
    grad_blocks = grad_in.reshape(num_blocks, block_rows, groups, per_group, head_dim)

    def attend_block(carried, pieces):
        key_acc, value_acc = carried
        query_piece, grad_piece = pieces
        scores = product("qgrd,cgd->grqc", query_piece, key_rot) * score_scale
        row_max = jnp.max(scores, axis=-1, keepdims=True)
        shifted = jnp.exp(scores - row_max)
        attn_prob = shifted / jnp.sum(shifted, axis=-1, keepdims=True)
        prob_low = attn_prob.astype(jnp.bfloat16)
        prob_grad = product("qgrd,cgd->grqc", grad_piece, value_input)
        row_dot = jnp.sum(attn_prob * prob_grad, axis=-1, keepdims=True)
        score_grad = (attn_prob * (prob_grad - row_dot) * score_scale).astype(jnp.bfloat16)
        dq_piece = product("grqc,cgd->qgrd", score_grad, key_rot)
        key_acc = key_acc + product("grqc,qgrd->cgd", score_grad, query_piece)
        value_acc = value_acc + product("grqc,qgrd->cgd", prob_low, grad_piece)
        return ((key_acc, value_acc), dq_piece)

    empty_acc = jnp.zeros((token_length, groups, head_dim), jnp.float32)
    (key_rot_grad, value_acc), query_rot_grad = lax.scan(
        attend_block, (empty_acc, empty_acc), (query_blocks, grad_blocks)
    )
    query_rot_grad = query_rot_grad.reshape(token_length, groups, per_group, head_dim)
    query_grad = norm_back(
        query_f, query_inv, rotate_back(query_rot_grad, cos_four, sin_four), query_gain
    ).astype(jnp.bfloat16)
    key_portion = norm_back(
        key_f, key_inv, rotate_back(key_rot_grad, cos_three, sin_three), key_gain
    ).astype(jnp.bfloat16)
    return (query_grad, key_portion, value_acc.astype(jnp.bfloat16))


def generic_device(
    inputs, queries, keys, values, out_grad, query_gain, key_gain, key_matrix, value_matrix
):
    sp_count = lax.axis_size("sp")
    dp_count = lax.axis_size("dp")
    token_row_block = inputs.shape[1]
    token_length = token_row_block * sp_count
    local_heads = QUERY_HEADS // sp_count
    portion_heads = min(local_heads, QUERY_HEADS // KEY_VALUE_HEADS)
    kv_here = local_heads // portion_heads
    group_copies = QUERY_HEADS // KEY_VALUE_HEADS // portion_heads
    key_value_width = KEY_VALUE_HEADS * HEAD_CHANNELS
    key_positions = jnp.repeat(
        keys[0].reshape(token_row_block, KEY_VALUE_HEADS, HEAD_CHANNELS), group_copies, axis=1
    ).reshape(token_row_block, key_value_width * group_copies)
    value_positions = jnp.repeat(
        values[0].reshape(token_row_block, KEY_VALUE_HEADS, HEAD_CHANNELS), group_copies, axis=1
    ).reshape(token_row_block, key_value_width * group_copies)
    grad_heads, query_heads, key_heads, value_heads = (
        lax.all_to_all(out_grad[0], "sp", split_axis=1, concat_axis=0, tiled=True),
        lax.all_to_all(queries[0], "sp", split_axis=1, concat_axis=0, tiled=True),
        lax.all_to_all(key_positions, "sp", split_axis=1, concat_axis=0, tiled=True),
        lax.all_to_all(value_positions, "sp", split_axis=1, concat_axis=0, tiled=True),
    )
    cos_tab, sin_tab = rotary_tables(token_length)
    query_part, key_portion, value_portion = head_grads(
        query_heads.reshape(token_length, kv_here, portion_heads, HEAD_CHANNELS),
        key_heads.reshape(token_length, kv_here, HEAD_CHANNELS),
        value_heads.reshape(token_length, kv_here, HEAD_CHANNELS),
        grad_heads.reshape(token_length, kv_here, portion_heads, HEAD_CHANNELS),
        query_gain,
        key_gain,
        cos_tab,
        sin_tab,
        min(512, token_length),
    )
    query_tokens, key_token_rows, value_token_rows = (
        lax.all_to_all(
            query_part.reshape(token_length, local_heads * HEAD_CHANNELS),
            "sp",
            split_axis=0,
            concat_axis=1,
            tiled=True,
        ),
        lax.all_to_all(
            key_portion.reshape(token_length, kv_here * HEAD_CHANNELS),
            "sp",
            split_axis=0,
            concat_axis=1,
            tiled=True,
        ),
        lax.all_to_all(
            value_portion.reshape(token_length, kv_here * HEAD_CHANNELS),
            "sp",
            split_axis=0,
            concat_axis=1,
            tiled=True,
        ),
    )
    key_gradient = (
        key_token_rows.reshape(token_row_block, KEY_VALUE_HEADS, group_copies, HEAD_CHANNELS)
        .astype(jnp.float32)
        .sum(axis=2)
        .astype(jnp.bfloat16)
    )
    value_gradient = (
        value_token_rows.reshape(token_row_block, KEY_VALUE_HEADS, group_copies, HEAD_CHANNELS)
        .astype(jnp.float32)
        .sum(axis=2)
        .astype(jnp.bfloat16)
    )
    projection_gradient = jnp.concatenate(
        [
            key_gradient.reshape(token_row_block, key_value_width),
            value_gradient.reshape(token_row_block, key_value_width),
        ],
        axis=1,
    )
    joined_weight = jnp.concatenate([key_matrix, value_matrix], axis=1)
    input_grad = lax.dot_general(
        projection_gradient,
        lax.all_gather(joined_weight, "dp", axis=0, tiled=True),
        (((1,), (1,)), ((), ())),
        preferred_element_type=jnp.float32,
    ).astype(jnp.bfloat16)
    token_in = inputs[0]
    width = inputs.shape[2]
    row_share = width // (sp_count * dp_count)
    permuted = (
        token_in.reshape(token_row_block, dp_count, sp_count, row_share)
        .transpose(0, 2, 1, 3)
        .reshape(token_row_block, width)
    )
    share_cols = lax.all_to_all(permuted, "sp", split_axis=1, concat_axis=0, tiled=True)
    all_grads = lax.all_gather(projection_gradient, "sp", axis=0, tiled=True)
    grad_piece = lax.psum_scatter(
        lax.dot_general(
            share_cols, all_grads, (((0,), (0,)), ((), ())), preferred_element_type=jnp.float32
        ).astype(jnp.bfloat16),
        "dp",
        scatter_dimension=0,
        tiled=True,
    ).astype(jnp.float32)
    weight_grad = lax.all_gather(grad_piece, "sp", axis=0, tiled=True)
    return (
        input_grad[None],
        query_tokens[None],
        weight_grad[:, :key_value_width],
        weight_grad[:, key_value_width:],
    )


bf16 = jnp.bfloat16
f32 = jnp.float32


def dot(first_op, second_op, first_dim, second_dim):
    return lax.dot_general(
        first_op, second_op, (((first_dim,), (second_dim,)), ((), ())), preferred_element_type=f32
    )


MIB = 1024 * 1024


def in_vmem(value):
    return pltpu.with_memory_space_constraint(value, pltpu.VMEM)


def kernel_call(body, out_shape, scratch, args, flops=0, limit=12 * MIB):
    vmem = pl.BlockSpec(memory_space=pltpu.VMEM)
    return pl.pallas_call(
        body,
        out_shape=out_shape,
        in_specs=[vmem] * len(args),
        out_specs=[vmem] * len(out_shape),
        scratch_shapes=scratch,
        cost_estimate=pl.CostEstimate(flops=flops, bytes_accessed=0, transcendentals=0),
        compiler_params=pltpu.CompilerParams(vmem_limit_bytes=limit),
    )(*[in_vmem(arg) for arg in args])


def held(shape, dtype=bf16):
    return pltpu.VMEM(shape, dtype)


def shape_of(shape, dtype=bf16):
    return jax.ShapeDtypeStruct(shape, dtype)


def swap_with(value, axis, k):
    count = lax.axis_size(axis)
    return lax.ppermute(value, axis, [(i, i ^ k) for i in range(count)])


def copy_call(body, out_shape, count, args):
    def run(*refs):
        sems = refs[-1]
        copies = [
            pltpu.make_async_copy(source, target, sems.at[i])
            for i, (source, target) in enumerate(body(*refs[:-1]))
        ]
        for copy in copies:
            copy.start()
        for copy in copies:
            copy.wait()

    return pl.pallas_call(
        run,
        out_shape=out_shape,
        in_specs=[pl.BlockSpec(memory_space=pltpu.HBM)] * len(args),
        out_specs=[pl.BlockSpec(memory_space=pltpu.VMEM)] * len(out_shape),
        scratch_shapes=[pltpu.SemaphoreType.DMA((count,))],
        compiler_params=pltpu.CompilerParams(vmem_limit_bytes=4 * MIB),
    )(*[pltpu.with_memory_space_constraint(arg, pltpu.HBM) for arg in args])


def lanes_of(half, width):
    return pl.ds(pl.multiple_of(half * width, 128), width)


def head_copies(refs, out, half, q_half, kv_half):
    pairs = []
    lo = 0
    for ref, width in zip(refs, (q_half, q_half, kv_half, kv_half)):
        pairs.append((ref.at[:, lanes_of(half, width)], out.at[:, lo : lo + width]))
        lo += width
    return pairs


def pack_heads(queries, keys, values, out_grad):
    rows, q_all = queries.shape
    q_half, kv_half = q_all // 2, keys.shape[1] // 2

    def body(q_ref, g_ref, k_ref, v_ref, mate, far, far_mate):
        bit = lax.axis_index("sp") % 2
        pairs = head_copies((q_ref, g_ref, k_ref, v_ref), mate, 1 - bit, q_half, kv_half)
        for out, half in ((far, bit), (far_mate, 1 - bit)):
            lanes = lanes_of(half, kv_half)
            pairs.append((k_ref.at[:, lanes], out.at[:, :kv_half]))
            pairs.append((v_ref.at[:, lanes], out.at[:, kv_half:]))
        return pairs

    return copy_call(
        body,
        [held((rows, 2 * q_half + 2 * kv_half))] + [held((rows, 2 * kv_half))] * 2,
        8,
        (queries, out_grad, keys, values),
    )


def pack_own(queries, keys, values, out_grad, key_matrix, value_matrix, small):
    rows, q_all = queries.shape
    q_half, kv_half = q_all // 2, keys.shape[1] // 2

    def body(q_ref, g_ref, k_ref, v_ref, wk_ref, wv_ref, *rest):
        own, weight = rest[len(small) : len(small) + 2]
        bit = lax.axis_index("sp") % 2
        pairs = head_copies((q_ref, g_ref, k_ref, v_ref), own, bit, q_half, kv_half)
        for d in range(2):
            cols = slice(d * kv_half, (d + 1) * kv_half)
            for ref, at in ((wk_ref, 2 * d), (wv_ref, 2 * d + 1)):
                pairs.append((ref.at[:, cols], weight.at[:, at * kv_half : (at + 1) * kv_half]))
        return pairs + list(zip(rest[: len(small)], rest[len(small) + 2 :]))

    return copy_call(
        body,
        [held((rows, 2 * q_half + 2 * kv_half)), held((key_matrix.shape[0], 4 * kv_half))]
        + [held(value.shape, value.dtype) for value in small],
        8 + len(small),
        (queries, out_grad, keys, values, key_matrix, value_matrix, *small),
    )


def turn_inputs(own, mate):
    rows, width = own.shape

    def body(own_ref, mate_ref, out):
        out[:, :rows] = own_ref[...].T
        out[:, rows:] = mate_ref[...].T

    return kernel_call(body, [held((width, 2 * rows))], [], (own, mate))[0]


def angle_tables(token_length):
    half_pairs = HEAD_CHANNELS // 4
    inv_freq = rope_base ** (-np.arange(half_pairs, dtype=np.float64) / half_pairs)
    inv_freq = inv_freq.astype(np.float32)
    channel = np.arange(2 * HEAD_CHANNELS)
    freq = inv_freq[(channel % HEAD_CHANNELS // 2) % half_pairs]
    sign = np.where(channel % 2 == 0, -1.0, 1.0).astype(np.float32)
    tables = []
    for count in (token_length // GRID, GRID):
        angles = (np.arange(count, dtype=np.float32)[:, None] * freq).astype(np.float64)
        tables += [np.cos(angles).astype(np.float32), (np.sin(angles) * sign).astype(np.float32)]
    return tables


class Rotation:
    def __init__(self, row_cos, row_sin, col_cos, col_sin):
        self.tables = (row_cos, row_sin, col_cos, col_sin)
        self.pair = 2 * HEAD_CHANNELS
        lane = lax.broadcasted_iota(jnp.int32, (GRID, self.pair), 1)
        self.even = lane % 2 == 0
        self.by_row = lane % HEAD_CHANNELS < HEAD_CHANNELS // 2
        seg_r = lax.broadcasted_iota(jnp.int32, (2 * self.pair, self.pair), 0)
        seg_c = lax.broadcasted_iota(jnp.int32, (2 * self.pair, self.pair), 1)
        same = seg_r // HEAD_CHANNELS % 2 == seg_c // HEAD_CHANNELS
        self.seg = jnp.where(same, 1.0 / HEAD_CHANNELS, 0.0).astype(bf16)

    def head_mean(self, product_f):
        high = product_f.astype(bf16)
        low = (product_f - high.astype(f32)).astype(bf16)
        return dot(jnp.concatenate([high, low], axis=1), self.seg, 1, 0)

    def swap(self, value):
        left, right = pltpu.roll(value, self.pair - 1, 1), pltpu.roll(value, 1, 1)
        return jnp.where(self.even, left, right)

    def angles_of(self, r):
        row_cos, row_sin, col_cos, col_sin = self.tables
        cos = jnp.where(self.by_row, row_cos[pl.ds(r, 1), :], col_cos[...])
        sin = jnp.where(self.by_row, row_sin[pl.ds(r, 1), :], col_sin[...])
        return cos, sin

    def forward(self, value, gain, cos, sin):
        inv = lax.rsqrt(self.head_mean(value * value) + norm_eps)
        normed = value * inv * gain
        return inv, (normed * cos + self.swap(normed) * sin).astype(bf16)

    def backward(self, value, inv, grad, gain, cos, sin):
        weighted = (grad * cos - self.swap(grad) * sin) * gain
        inner = self.head_mean(weighted * value)
        return inv * (weighted - value * inv * inv * inner)


def split_halves(value, upper, half, own_out, far_out):
    own_out[...] = value[pl.ds(pl.multiple_of(upper * half, half), half), :]
    far_out[...] = value[pl.ds(pl.multiple_of((1 - upper) * half, half), half), :].astype(bf16)


def attention_values(own, mate, far, far_mate, gains, tables):
    rows, width = own.shape
    k_width = far.shape[1] // 2
    q_width = width // 2 - k_width
    pair = 2 * HEAD_CHANNELS
    heads = q_width // HEAD_CHANNELS
    groups = k_width // HEAD_CHANNELS
    per_group = heads // groups
    half = 2 * rows
    tokens = 4 * rows

    def body(*refs):
        own_ref, mate_ref, far_ref, far_mate_ref, qg_ref, kg_ref = refs[:6]
        pv_own, pv_far, probs, qh, gh, kr, vv, q_inv, k_inv, q_tok, kv_tok, dv_sc = refs[10:]
        me = lax.axis_index("sp")
        bit = me % 2
        upper = me // 2
        q_tok[pl.ds(pl.multiple_of(bit * rows, rows), rows), :] = own_ref[:, : 2 * q_width]
        q_tok[pl.ds(pl.multiple_of((1 - bit) * rows, rows), rows), :] = mate_ref[:, : 2 * q_width]
        for k, block in enumerate(
            (own_ref[:, 2 * q_width :], mate_ref[:, 2 * q_width :], far_ref[...], far_mate_ref[...])
        ):
            kv_tok[pl.ds(pl.multiple_of((me ^ k) * rows, rows), rows), :] = block
        turn = Rotation(*refs[6:10])
        q_gain = jnp.concatenate([qg_ref[...], qg_ref[...]], axis=1)
        k_gain = jnp.concatenate([kg_ref[...], kg_ref[...]], axis=1)
        q_rows = half // GRID
        for r in range(tokens // GRID):
            at = slice(r * GRID, (r + 1) * GRID)
            cos, sin = turn.angles_of(r)
            for lo in range(0, k_width, pair):
                part = slice(lo, lo + pair)
                inv, turned = turn.forward(kv_tok[at, part].astype(f32), k_gain, cos, sin)
                k_inv[at, part] = inv
                for u in range(2):
                    g = lo // HEAD_CHANNELS + u
                    kr[g, at, :] = turned[:, u * HEAD_CHANNELS : (u + 1) * HEAD_CHANNELS]
                    begin = k_width + g * HEAD_CHANNELS
                    vv[g, at, :] = kv_tok[at, begin : begin + HEAD_CHANNELS]
        for r in range(q_rows):
            at = slice(r * GRID, (r + 1) * GRID)
            cos, sin = turn.angles_of(upper * q_rows + r)
            for lo in range(0, q_width, pair):
                part = slice(lo, lo + pair)
                inv, turned = turn.forward(q_tok[at, part].astype(f32), q_gain, cos, sin)
                q_inv[at, part] = inv
                grad = q_tok[at, q_width + lo : q_width + lo + pair]
                for u in range(2):
                    lanes = slice(u * HEAD_CHANNELS, (u + 1) * HEAD_CHANNELS)
                    qh[lo // HEAD_CHANNELS + u, at, :] = turned[:, lanes]
                    gh[lo // HEAD_CHANNELS + u, at, :] = grad[:, lanes]
        for g in range(groups):
            key_rot = kr[g]
            for h in range(g * per_group, (g + 1) * per_group):
                scores = dot(key_rot, qh[h], 1, 1)
                top = jnp.max(scores, axis=0, keepdims=True)
                expo = jnp.exp((scores - top) * score_scale)
                prob = expo * (1.0 / jnp.sum(expo, axis=0, keepdims=True))
                probs[h] = prob
                dv = dot(prob.astype(bf16), gh[h], 1, 0)
                value_acc = dv if h == g * per_group else value_acc + dv
            dv_sc[:, g * HEAD_CHANNELS : (g + 1) * HEAD_CHANNELS] = value_acc
        split_halves(dv_sc, upper, half, pv_own, pv_far)

    outs = kernel_call(
        body,
        [
            held((half, k_width), f32),
            held((half, k_width)),
            held((heads, tokens, half), f32),
            held((heads, half, HEAD_CHANNELS)),
            held((heads, half, HEAD_CHANNELS)),
            held((groups, tokens, HEAD_CHANNELS)),
            held((groups, tokens, HEAD_CHANNELS)),
            held((half, q_width), f32),
            held((tokens, k_width), f32),
            held((half, 2 * q_width)),
            held((tokens, 2 * k_width)),
        ],
        [pltpu.VMEM((tokens, k_width), f32)],
        (own, mate, far, far_mate, *gains, *tables),
        flops=4 * heads * half * tokens * HEAD_CHANNELS,
        limit=20 * MIB,
    )
    return outs[0], outs[1], outs[2:]


def attention_keys(state, gains, tables):
    probs, _, _, kr, _, q_inv, k_inv, _, _ = state
    heads, tokens, half = probs.shape
    rows = half // 2
    groups = kr.shape[0]
    per_group = heads // groups
    q_width, k_width = q_inv.shape[1], k_inv.shape[1]
    pair = 2 * HEAD_CHANNELS

    def body(*refs):
        probs, qh, gh, kr, vv, q_inv, k_inv, q_tok, kv_tok, qg_ref, kg_ref = refs[:11]
        dq_own, dq_mate, pk_own, pk_far, dq_sc, dk_sc, dq_out, p_sc = refs[15:]
        me = lax.axis_index("sp")
        bit = me % 2
        upper = me // 2
        turn = Rotation(*refs[11:15])
        q_gain = jnp.concatenate([qg_ref[...], qg_ref[...]], axis=1)
        k_gain = jnp.concatenate([kg_ref[...], kg_ref[...]], axis=1)
        q_rows = half // GRID
        for g in range(groups):
            key_rot = kr[g]
            value_in = vv[g]
            for h in range(g * per_group, (g + 1) * per_group):
                prob = probs[h]
                prob_grad = dot(value_in, gh[h], 1, 1)
                row_dot = jnp.sum(prob * prob_grad, axis=0, keepdims=True)
                score_grad = (prob * (prob_grad - row_dot)).astype(bf16)
                dk = dot(score_grad, qh[h], 1, 0)
                dq_t = dot(key_rot, score_grad, 0, 0)
                dq_sc[:, h * HEAD_CHANNELS : (h + 1) * HEAD_CHANNELS] = dq_t.T * score_scale
                key_acc = dk if h == g * per_group else key_acc + dk
            dk_sc[:, g * HEAD_CHANNELS : (g + 1) * HEAD_CHANNELS] = key_acc * score_scale
        for r in range(tokens // GRID):
            at = slice(r * GRID, (r + 1) * GRID)
            cos, sin = turn.angles_of(r)
            for lo in range(0, k_width, pair):
                part = slice(lo, lo + pair)
                value = kv_tok[at, part].astype(f32)
                p_sc[at, part] = turn.backward(
                    value, k_inv[at, part], dk_sc[at, part], k_gain, cos, sin
                )
        split_halves(p_sc, upper, half, pk_own, pk_far)
        for r in range(q_rows):
            at = slice(r * GRID, (r + 1) * GRID)
            cos, sin = turn.angles_of(upper * q_rows + r)
            for lo in range(0, q_width, pair):
                part = slice(lo, lo + pair)
                value = q_tok[at, part].astype(f32)
                result = turn.backward(value, q_inv[at, part], dq_sc[at, part], q_gain, cos, sin)
                dq_out[at, part] = result.astype(bf16)
        dq_own[...] = dq_out[pl.ds(pl.multiple_of(bit * rows, rows), rows), :]
        dq_mate[...] = dq_out[pl.ds(pl.multiple_of((1 - bit) * rows, rows), rows), :]

    return kernel_call(
        body,
        [held((rows, q_width))] * 2 + [held((half, k_width), f32), held((half, k_width))],
        [
            pltpu.VMEM((half, q_width), f32),
            pltpu.VMEM((tokens, k_width), f32),
            pltpu.VMEM((half, q_width), bf16),
            pltpu.VMEM((tokens, k_width), f32),
        ],
        (*state, *gains, *tables),
        flops=6 * heads * half * tokens * HEAD_CHANNELS,
        limit=20 * MIB,
    )


def weight_partials(turned, p_own, p_far, extra, dp_count):
    feats, half = turned.shape
    rows, cols = half // 2, p_own.shape[1]
    share = feats // dp_count
    chips = dp_count // 2

    def body(x_ref, po_ref, pf_ref, *rest):
        mine_out, mate_out, own_out, send_out, p_sc = rest[len(extra) :]
        bit = lax.axis_index("sp") % 2
        mine = lax.axis_index("dp")
        p_sc[...] = (po_ref[...] + pf_ref[...].astype(f32)).astype(bf16)
        p_mine = p_sc[pl.ds(pl.multiple_of(bit * rows, rows), rows), :]
        p_mate = p_sc[pl.ds(pl.multiple_of((1 - bit) * rows, rows), rows), :]
        mine_out[...] = p_mine
        mate_out[:, :cols] = p_mate
        lo = cols
        for ref in rest[: len(extra)]:
            mate_out[:, lo : lo + ref.shape[1]] = ref[...]
            lo += ref.shape[1]
        p_all = jnp.concatenate([p_mine, p_mate], axis=0)
        for out, flip in ((send_out, 1), (own_out, 0)):
            for m in range(chips):
                start = pl.multiple_of((mine ^ (2 * m + flip)) * share, share)
                out[m] = dot(x_ref[pl.ds(start, share), :], p_all, 1, 0).astype(bf16)

    return kernel_call(
        body,
        [held((rows, cols)), held((rows, cols + sum(value.shape[1] for value in extra)))]
        + [held((chips, share, cols))] * 2,
        [pltpu.VMEM((half, cols), bf16)],
        (turned, p_own, p_far, *extra),
        flops=2 * feats * half * cols,
    )


def sum_cores(own, received):
    chips, share, cols = own.shape

    def body(own_ref, got_ref, first, *rest):
        first[...] = own_ref[0].astype(f32) + got_ref[0].astype(f32)
        for m, out in enumerate(rest, 1):
            out[...] = (own_ref[m].astype(f32) + got_ref[m].astype(f32)).astype(bf16)

    return kernel_call(
        body, [held((share, cols), f32)] + [held((share, cols))] * (chips - 1), [], (own, received)
    )


def sum_chips(first, received):
    def body(*refs):
        total = refs[0][...]
        for ref in refs[1:-1]:
            total = total + ref[...].astype(f32)
        refs[-1][...] = total.astype(bf16)

    return kernel_call(body, [held(first.shape)], [], (first, *received))[0]


def join_weight_grad(own, mate, far, far_mate):
    rows, cols = own.shape

    def body(own_ref, mate_ref, far_ref, far_mate_ref, out, scratch, sem):
        even = lax.axis_index("sp") % 2 == 0
        here = own_ref[...].astype(f32) + far_ref[...].astype(f32)
        there = mate_ref[...].astype(f32) + far_mate_ref[...].astype(f32)
        scratch[:, :cols] = jnp.where(even, here, there)
        scratch[:, cols:] = jnp.where(even, there, here)
        copy = pltpu.make_async_copy(scratch, out, sem)
        copy.start()
        copy.wait()

    return pl.pallas_call(
        body,
        out_shape=shape_of((rows, 2 * cols), f32),
        in_specs=[pl.BlockSpec(memory_space=pltpu.VMEM)] * 4,
        out_specs=pl.BlockSpec(memory_space=pltpu.HBM),
        scratch_shapes=[pltpu.VMEM((rows, 2 * cols), f32), pltpu.SemaphoreType.DMA],
        compiler_params=pltpu.CompilerParams(vmem_limit_bytes=4 * MIB),
    )(*[in_vmem(piece) for piece in (own, mate, far, far_mate)])


def token_outputs(k_mine, v_mine, from_mate, weight_pieces, dq_own):
    rows, cols = k_mine.shape
    q_half = dq_own.shape[1]
    dp_count = len(weight_pieces)
    w_rows = weight_pieces[0].shape[0]

    def body(k_ref, v_ref, mate_ref, dq_ref, *rest):
        w_refs = rest[:dp_count]
        x_out, q_out, p_buf, out_buf, q_buf = rest[dp_count:]
        bit = lax.axis_index("sp") % 2
        mine = lax.axis_index("dp")
        p_buf[bit] = jnp.concatenate([k_ref[...], v_ref[...]], axis=1)
        p_buf[1 - bit] = mate_ref[:, : 2 * cols]
        q_buf[bit] = dq_ref[...]
        q_buf[1 - bit] = mate_ref[:, 2 * cols :]
        for d in range(2):
            q_out[:, d * q_half : (d + 1) * q_half] = q_buf[d]
        left = jnp.concatenate([p_buf[0], p_buf[1]], axis=1)
        for m in range(dp_count):
            out_buf[mine ^ m] = dot(left, w_refs[m][...], 1, 1).astype(bf16)
        for j in range(dp_count):
            x_out[:, j * w_rows : (j + 1) * w_rows] = out_buf[j]

    return kernel_call(
        body,
        [shape_of((rows, dp_count * w_rows)), shape_of((rows, 2 * q_half))],
        [
            pltpu.VMEM((2, rows, 2 * cols), bf16),
            pltpu.VMEM((dp_count, rows, w_rows), bf16),
            pltpu.VMEM((2, rows, q_half), bf16),
        ],
        (k_mine, v_mine, from_mate, dq_own, *weight_pieces),
        flops=8 * rows * dp_count * w_rows * cols,
    )


def fast_device(
    inputs, queries, keys, values, out_grad, query_gain, key_gain, key_matrix, value_matrix
):
    return fast_body(
        inputs[0],
        queries[0],
        keys[0],
        values[0],
        out_grad[0],
        query_gain,
        key_gain,
        key_matrix,
        value_matrix,
    )


def fast_body(
    inputs, queries, keys, values, out_grad, query_gain, key_gain, key_matrix, value_matrix
):
    dp_count = lax.axis_size("dp")
    chips = dp_count // 2
    mate, far, far_mate = pack_heads(queries, keys, values, out_grad)
    mate = swap_with(mate, "sp", 1)
    far = swap_with(far, "sp", 2)
    far_mate = swap_with(far_mate, "sp", 3)
    tables = [jnp.asarray(table) for table in angle_tables(4 * inputs.shape[0])]
    own, joined_weight, *small = pack_own(
        queries,
        keys,
        values,
        out_grad,
        key_matrix,
        value_matrix,
        [query_gain[None], key_gain[None], *tables],
    )
    gains, tables = small[:2], small[2:]
    weight_pieces = [joined_weight] + [
        swap_with(joined_weight, "dp", m) for m in range(1, dp_count)
    ]
    mate_inputs = swap_with(inputs, "sp", 1)
    v_own, v_far, state = attention_values(own, mate, far, far_mate, gains, tables)
    v_far = swap_with(v_far, "sp", 2)
    dq_own, dq_mate, k_own, k_far = attention_keys(state, gains, tables)
    k_far = swap_with(k_far, "sp", 2)
    turned = turn_inputs(inputs, mate_inputs)

    def weight_grad(p_own, p_far, extra):
        mine, there, blocks, sent = weight_partials(turned, p_own, p_far, extra, dp_count)
        first, *rest = sum_cores(blocks, swap_with(sent, "dp", 1))
        received = [swap_with(rest[m - 1], "dp", 2 * m) for m in range(1, chips)]
        total = sum_chips(first, received)
        others = [swap_with(total, "sp", k) for k in range(1, 4)]
        return mine, there, join_weight_grad(total, *others)

    v_mine, v_there, value_weight = weight_grad(v_own, v_far, ())
    k_mine, there, key_weight = weight_grad(k_own, k_far, (v_there, dq_mate))
    from_mate = swap_with(there, "sp", 1)
    input_grad, query_grad = token_outputs(k_mine, v_mine, from_mate, weight_pieces, dq_own)
    return input_grad[None], query_grad[None], key_weight, value_weight


def solution(mesh):
    sp_count, dp_count = mesh.shape["sp"], mesh.shape["dp"]
    fast = sp_count == 4 and dp_count & (dp_count - 1) == 0
    return jax.shard_map(
        fast_device if fast else generic_device,
        mesh=mesh,
        in_specs=(
            P("dp", "sp", None),
            P("dp", "sp", None),
            P("dp", "sp", None),
            P("dp", "sp", None),
            P("dp", "sp", None),
            P(),
            P(),
            P("dp", None),
            P("dp", None),
        ),
        out_specs=(P("dp", "sp", None), P("dp", "sp", None), P("dp", None), P("dp", None)),
        check_vma=False,
    )
```

```python
import jax
import jax.numpy as jnp
import numpy as np
from jax import lax
from jax.experimental import pallas as pl
from jax.experimental.pallas import tpu as pltpu
from jax.sharding import PartitionSpec as P

QUERY_HEADS = 16
KEY_VALUE_HEADS = 4
HEAD_CHANNELS = 64
GRID = 64


rope_base = 10000.0
norm_eps = 0.5
score_scale = 0.125


def product(pattern, first_op, second_op):
    return jnp.einsum(pattern, first_op, second_op, preferred_element_type=jnp.float32)


def rotary_tables(token_length):
    position = jnp.arange(token_length, dtype=jnp.int32)
    grid_row = (position // GRID).astype(jnp.float32)
    grid_col = (position % GRID).astype(jnp.float32)
    half_pairs = HEAD_CHANNELS // 4
    inv_freq = rope_base ** (-jnp.arange(half_pairs, dtype=jnp.float32) / half_pairs)
    angles = jnp.concatenate([grid_row[:, None] * inv_freq, grid_col[:, None] * inv_freq], axis=1)
    return (jnp.cos(angles), jnp.sin(angles))


def rotate(vector, cos_tab, sin_tab):
    even_part = vector[..., 0::2]
    odd_part = vector[..., 1::2]
    turned = jnp.stack(
        [even_part * cos_tab - odd_part * sin_tab, even_part * sin_tab + odd_part * cos_tab],
        axis=-1,
    )
    return turned.reshape(vector.shape)


def rotate_back(cotangent, cos_tab, sin_tab):
    even_part = cotangent[..., 0::2]
    odd_part = cotangent[..., 1::2]
    turned = jnp.stack(
        [even_part * cos_tab + odd_part * sin_tab, odd_part * cos_tab - even_part * sin_tab],
        axis=-1,
    )
    return turned.reshape(cotangent.shape)


def inverse_rms(vector):
    return lax.rsqrt(jnp.mean(vector * vector, axis=-1, keepdims=True) + norm_eps)


def norm_back(vector, inv_scale, cotangent, gain_vec):
    weighted = cotangent * gain_vec
    inner_mean = jnp.mean(weighted * vector, axis=-1, keepdims=True)
    return inv_scale * (weighted - vector * inv_scale * inv_scale * inner_mean)


def head_grads(
    query_in, key_input, value_input, grad_in, query_gain, key_gain, cos_tab, sin_tab, block_rows
):
    token_length, groups, per_group, head_dim = query_in.shape
    cos_four = cos_tab[:, None, None, :]
    sin_four = sin_tab[:, None, None, :]
    cos_three = cos_tab[:, None, :]
    sin_three = sin_tab[:, None, :]
    query_f = query_in.astype(jnp.float32)
    query_inv = inverse_rms(query_f)
    query_rot = rotate(query_f * query_inv * query_gain, cos_four, sin_four).astype(jnp.bfloat16)
    key_f = key_input.astype(jnp.float32)
    key_inv = inverse_rms(key_f)
    key_rot = rotate(key_f * key_inv * key_gain, cos_three, sin_three).astype(jnp.bfloat16)
    num_blocks = token_length // block_rows
    query_blocks = query_rot.reshape(num_blocks, block_rows, groups, per_group, head_dim)
    grad_blocks = grad_in.reshape(num_blocks, block_rows, groups, per_group, head_dim)

    def attend_block(carried, pieces):
        key_acc, value_acc = carried
        query_piece, grad_piece = pieces
        scores = product("qgrd,cgd->grqc", query_piece, key_rot) * score_scale
        row_max = jnp.max(scores, axis=-1, keepdims=True)
        shifted = jnp.exp(scores - row_max)
        attn_prob = shifted / jnp.sum(shifted, axis=-1, keepdims=True)
        prob_low = attn_prob.astype(jnp.bfloat16)
        prob_grad = product("qgrd,cgd->grqc", grad_piece, value_input)
        row_dot = jnp.sum(attn_prob * prob_grad, axis=-1, keepdims=True)
        score_grad = (attn_prob * (prob_grad - row_dot) * score_scale).astype(jnp.bfloat16)
        dq_piece = product("grqc,cgd->qgrd", score_grad, key_rot)
        key_acc = key_acc + product("grqc,qgrd->cgd", score_grad, query_piece)
        value_acc = value_acc + product("grqc,qgrd->cgd", prob_low, grad_piece)
        return ((key_acc, value_acc), dq_piece)

    empty_acc = jnp.zeros((token_length, groups, head_dim), jnp.float32)
    (key_rot_grad, value_acc), query_rot_grad = lax.scan(
        attend_block, (empty_acc, empty_acc), (query_blocks, grad_blocks)
    )
    query_rot_grad = query_rot_grad.reshape(token_length, groups, per_group, head_dim)
    query_grad = norm_back(
        query_f, query_inv, rotate_back(query_rot_grad, cos_four, sin_four), query_gain
    ).astype(jnp.bfloat16)
    key_portion = norm_back(
        key_f, key_inv, rotate_back(key_rot_grad, cos_three, sin_three), key_gain
    ).astype(jnp.bfloat16)
    return (query_grad, key_portion, value_acc.astype(jnp.bfloat16))


def generic_device(
    inputs, queries, keys, values, out_grad, query_gain, key_gain, key_matrix, value_matrix
):
    sp_count = lax.axis_size("sp")
    dp_count = lax.axis_size("dp")
    token_row_block = inputs.shape[1]
    token_length = token_row_block * sp_count
    local_heads = QUERY_HEADS // sp_count
    portion_heads = min(local_heads, QUERY_HEADS // KEY_VALUE_HEADS)
    kv_here = local_heads // portion_heads
    group_copies = QUERY_HEADS // KEY_VALUE_HEADS // portion_heads
    key_value_width = KEY_VALUE_HEADS * HEAD_CHANNELS
    key_positions = jnp.repeat(
        keys[0].reshape(token_row_block, KEY_VALUE_HEADS, HEAD_CHANNELS), group_copies, axis=1
    ).reshape(token_row_block, key_value_width * group_copies)
    value_positions = jnp.repeat(
        values[0].reshape(token_row_block, KEY_VALUE_HEADS, HEAD_CHANNELS), group_copies, axis=1
    ).reshape(token_row_block, key_value_width * group_copies)
    grad_heads, query_heads, key_heads, value_heads = (
        lax.all_to_all(out_grad[0], "sp", split_axis=1, concat_axis=0, tiled=True),
        lax.all_to_all(queries[0], "sp", split_axis=1, concat_axis=0, tiled=True),
        lax.all_to_all(key_positions, "sp", split_axis=1, concat_axis=0, tiled=True),
        lax.all_to_all(value_positions, "sp", split_axis=1, concat_axis=0, tiled=True),
    )
    cos_tab, sin_tab = rotary_tables(token_length)
    query_part, key_portion, value_portion = head_grads(
        query_heads.reshape(token_length, kv_here, portion_heads, HEAD_CHANNELS),
        key_heads.reshape(token_length, kv_here, HEAD_CHANNELS),
        value_heads.reshape(token_length, kv_here, HEAD_CHANNELS),
        grad_heads.reshape(token_length, kv_here, portion_heads, HEAD_CHANNELS),
        query_gain,
        key_gain,
        cos_tab,
        sin_tab,
        min(512, token_length),
    )
    query_tokens, key_token_rows, value_token_rows = (
        lax.all_to_all(
            query_part.reshape(token_length, local_heads * HEAD_CHANNELS),
            "sp",
            split_axis=0,
            concat_axis=1,
            tiled=True,
        ),
        lax.all_to_all(
            key_portion.reshape(token_length, kv_here * HEAD_CHANNELS),
            "sp",
            split_axis=0,
            concat_axis=1,
            tiled=True,
        ),
        lax.all_to_all(
            value_portion.reshape(token_length, kv_here * HEAD_CHANNELS),
            "sp",
            split_axis=0,
            concat_axis=1,
            tiled=True,
        ),
    )
    key_gradient = (
        key_token_rows.reshape(token_row_block, KEY_VALUE_HEADS, group_copies, HEAD_CHANNELS)
        .astype(jnp.float32)
        .sum(axis=2)
        .astype(jnp.bfloat16)
    )
    value_gradient = (
        value_token_rows.reshape(token_row_block, KEY_VALUE_HEADS, group_copies, HEAD_CHANNELS)
        .astype(jnp.float32)
        .sum(axis=2)
        .astype(jnp.bfloat16)
    )
    projection_gradient = jnp.concatenate(
        [
            key_gradient.reshape(token_row_block, key_value_width),
            value_gradient.reshape(token_row_block, key_value_width),
        ],
        axis=1,
    )
    joined_weight = jnp.concatenate([key_matrix, value_matrix], axis=1)
    input_grad = lax.dot_general(
        projection_gradient,
        lax.all_gather(joined_weight, "dp", axis=0, tiled=True),
        (((1,), (1,)), ((), ())),
        preferred_element_type=jnp.float32,
    ).astype(jnp.bfloat16)
    token_in = inputs[0]
    width = inputs.shape[2]
    row_share = width // (sp_count * dp_count)
    permuted = (
        token_in.reshape(token_row_block, dp_count, sp_count, row_share)
        .transpose(0, 2, 1, 3)
        .reshape(token_row_block, width)
    )
    share_cols = lax.all_to_all(permuted, "sp", split_axis=1, concat_axis=0, tiled=True)
    all_grads = lax.all_gather(projection_gradient, "sp", axis=0, tiled=True)
    grad_piece = lax.psum_scatter(
        lax.dot_general(
            share_cols, all_grads, (((0,), (0,)), ((), ())), preferred_element_type=jnp.float32
        ).astype(jnp.bfloat16),
        "dp",
        scatter_dimension=0,
        tiled=True,
    ).astype(jnp.float32)
    weight_grad = lax.all_gather(grad_piece, "sp", axis=0, tiled=True)
    return (
        input_grad[None],
        query_tokens[None],
        weight_grad[:, :key_value_width],
        weight_grad[:, key_value_width:],
    )


bf16 = jnp.bfloat16
f32 = jnp.float32


def dot(first_op, second_op, first_dim, second_dim):
    return lax.dot_general(
        first_op, second_op, (((first_dim,), (second_dim,)), ((), ())), preferred_element_type=f32
    )


MIB = 1024 * 1024


def in_vmem(value):
    return pltpu.with_memory_space_constraint(value, pltpu.VMEM)


def kernel_call(body, out_shape, scratch, args, flops=0, limit=12 * MIB):
    vmem = pl.BlockSpec(memory_space=pltpu.VMEM)
    return pl.pallas_call(
        body,
        out_shape=out_shape,
        in_specs=[vmem] * len(args),
        out_specs=[vmem] * len(out_shape),
        scratch_shapes=scratch,
        cost_estimate=pl.CostEstimate(flops=flops, bytes_accessed=0, transcendentals=0),
        compiler_params=pltpu.CompilerParams(vmem_limit_bytes=limit),
    )(*[in_vmem(arg) for arg in args])


def held(shape, dtype=bf16):
    return pltpu.VMEM(shape, dtype)


def shape_of(shape, dtype=bf16):
    return jax.ShapeDtypeStruct(shape, dtype)


def swap_with(value, axis, k):
    count = lax.axis_size(axis)
    return lax.ppermute(value, axis, [(i, i ^ k) for i in range(count)])


def copy_call(body, out_shape, count, args):
    def run(*refs):
        sems = refs[-1]
        copies = [
            pltpu.make_async_copy(source, target, sems.at[i])
            for i, (source, target) in enumerate(body(*refs[:-1]))
        ]
        for copy in copies:
            copy.start()
        for copy in copies:
            copy.wait()

    return pl.pallas_call(
        run,
        out_shape=out_shape,
        in_specs=[pl.BlockSpec(memory_space=pltpu.HBM)] * len(args),
        out_specs=[pl.BlockSpec(memory_space=pltpu.VMEM)] * len(out_shape),
        scratch_shapes=[pltpu.SemaphoreType.DMA((count,))],
        compiler_params=pltpu.CompilerParams(vmem_limit_bytes=4 * MIB),
    )(*[pltpu.with_memory_space_constraint(arg, pltpu.HBM) for arg in args])


def lanes_of(half, width):
    return pl.ds(pl.multiple_of(half * width, 128), width)


def head_copies(refs, out, half, q_half, kv_half):
    pairs = []
    lo = 0
    for ref, width in zip(refs, (q_half, q_half, kv_half, kv_half)):
        pairs.append((ref.at[:, lanes_of(half, width)], out.at[:, lo : lo + width]))
        lo += width
    return pairs


def pack_heads(queries, keys, values, out_grad):
    rows, q_all = queries.shape
    q_half, kv_half = q_all // 2, keys.shape[1] // 2

    def body(q_ref, g_ref, k_ref, v_ref, mate, far, far_mate):
        bit = lax.axis_index("sp") % 2
        pairs = head_copies((q_ref, g_ref, k_ref, v_ref), mate, 1 - bit, q_half, kv_half)
        for out, half in ((far, bit), (far_mate, 1 - bit)):
            lanes = lanes_of(half, kv_half)
            pairs.append((k_ref.at[:, lanes], out.at[:, :kv_half]))
            pairs.append((v_ref.at[:, lanes], out.at[:, kv_half:]))
        return pairs

    return copy_call(
        body,
        [held((rows, 2 * q_half + 2 * kv_half))] + [held((rows, 2 * kv_half))] * 2,
        8,
        (queries, out_grad, keys, values),
    )


def pack_own(queries, keys, values, out_grad, key_matrix, value_matrix, small):
    rows, q_all = queries.shape
    q_half, kv_half = q_all // 2, keys.shape[1] // 2

    def body(q_ref, g_ref, k_ref, v_ref, wk_ref, wv_ref, *rest):
        own, weight = rest[len(small) : len(small) + 2]
        bit = lax.axis_index("sp") % 2
        pairs = head_copies((q_ref, g_ref, k_ref, v_ref), own, bit, q_half, kv_half)
        for d in range(2):
            cols = slice(d * kv_half, (d + 1) * kv_half)
            for ref, at in ((wk_ref, 2 * d), (wv_ref, 2 * d + 1)):
                pairs.append((ref.at[:, cols], weight.at[:, at * kv_half : (at + 1) * kv_half]))
        return pairs + list(zip(rest[: len(small)], rest[len(small) + 2 :]))

    return copy_call(
        body,
        [held((rows, 2 * q_half + 2 * kv_half)), held((key_matrix.shape[0], 4 * kv_half))]
        + [held(value.shape, value.dtype) for value in small],
        8 + len(small),
        (queries, out_grad, keys, values, key_matrix, value_matrix, *small),
    )


def turn_inputs(token_in):
    def body(x_ref, out):
        out[...] = x_ref[...].T

    return kernel_call(body, [held(token_in.shape[::-1])], [], (token_in,))[0]


def angle_tables(token_length):
    half_pairs = HEAD_CHANNELS // 4
    inv_freq = rope_base ** (-np.arange(half_pairs, dtype=np.float64) / half_pairs)
    inv_freq = inv_freq.astype(np.float32)
    channel = np.arange(2 * HEAD_CHANNELS)
    freq = inv_freq[(channel % HEAD_CHANNELS // 2) % half_pairs]
    sign = np.where(channel % 2 == 0, -1.0, 1.0).astype(np.float32)
    tables = []
    for count in (token_length // GRID, GRID):
        angles = (np.arange(count, dtype=np.float32)[:, None] * freq).astype(np.float64)
        tables += [np.cos(angles).astype(np.float32), (np.sin(angles) * sign).astype(np.float32)]
    return tables


class Rotation:
    def __init__(self, row_cos, row_sin, col_cos, col_sin):
        self.tables = (row_cos, row_sin, col_cos, col_sin)
        self.pair = 2 * HEAD_CHANNELS
        lane = lax.broadcasted_iota(jnp.int32, (GRID, self.pair), 1)
        self.even = lane % 2 == 0
        self.by_row = lane % HEAD_CHANNELS < HEAD_CHANNELS // 2
        seg_r = lax.broadcasted_iota(jnp.int32, (2 * self.pair, self.pair), 0)
        seg_c = lax.broadcasted_iota(jnp.int32, (2 * self.pair, self.pair), 1)
        same = seg_r // HEAD_CHANNELS % 2 == seg_c // HEAD_CHANNELS
        self.seg = jnp.where(same, 1.0 / HEAD_CHANNELS, 0.0).astype(bf16)

    def head_mean(self, product_f):
        high = product_f.astype(bf16)
        low = (product_f - high.astype(f32)).astype(bf16)
        return dot(jnp.concatenate([high, low], axis=1), self.seg, 1, 0)

    def swap(self, value):
        left, right = pltpu.roll(value, self.pair - 1, 1), pltpu.roll(value, 1, 1)
        return jnp.where(self.even, left, right)

    def angles_of(self, r):
        row_cos, row_sin, col_cos, col_sin = self.tables
        cos = jnp.where(self.by_row, row_cos[pl.ds(r, 1), :], col_cos[...])
        sin = jnp.where(self.by_row, row_sin[pl.ds(r, 1), :], col_sin[...])
        return cos, sin

    def forward(self, value, gain, cos, sin):
        inv = lax.rsqrt(self.head_mean(value * value) + norm_eps)
        normed = value * inv * gain
        return inv, (normed * cos + self.swap(normed) * sin).astype(bf16)

    def backward(self, value, inv, grad, gain, cos, sin):
        weighted = (grad * cos - self.swap(grad) * sin) * gain
        inner = self.head_mean(weighted * value)
        return inv * (weighted - value * inv * inv * inner)


def split_halves(value, upper, half, own_out, far_out):
    own_out[...] = value[pl.ds(pl.multiple_of(upper * half, half), half), :]
    far_out[...] = value[pl.ds(pl.multiple_of((1 - upper) * half, half), half), :].astype(bf16)


def attention_values(own, mate, far, far_mate, gains, tables):
    rows, width = own.shape
    k_width = far.shape[1] // 2
    q_width = width // 2 - k_width
    pair = 2 * HEAD_CHANNELS
    heads = q_width // HEAD_CHANNELS
    groups = k_width // HEAD_CHANNELS
    per_group = heads // groups
    half = 2 * rows
    tokens = 4 * rows

    def body(*refs):
        own_ref, mate_ref, far_ref, far_mate_ref, qg_ref, kg_ref = refs[:6]
        pv_own, pv_far, probs, qh, gh, kr, vv, q_inv, k_inv, q_tok, kv_tok, dv_sc = refs[10:]
        me = lax.axis_index("sp")
        bit = me % 2
        upper = me // 2
        q_tok[pl.ds(pl.multiple_of(bit * rows, rows), rows), :] = own_ref[:, : 2 * q_width]
        q_tok[pl.ds(pl.multiple_of((1 - bit) * rows, rows), rows), :] = mate_ref[:, : 2 * q_width]
        for k, block in enumerate(
            (own_ref[:, 2 * q_width :], mate_ref[:, 2 * q_width :], far_ref[...], far_mate_ref[...])
        ):
            kv_tok[pl.ds(pl.multiple_of((me ^ k) * rows, rows), rows), :] = block
        turn = Rotation(*refs[6:10])
        q_gain = jnp.concatenate([qg_ref[...], qg_ref[...]], axis=1)
        k_gain = jnp.concatenate([kg_ref[...], kg_ref[...]], axis=1)
        q_rows = half // GRID
        for r in range(tokens // GRID):
            at = slice(r * GRID, (r + 1) * GRID)
            cos, sin = turn.angles_of(r)
            for lo in range(0, k_width, pair):
                part = slice(lo, lo + pair)
                inv, turned = turn.forward(kv_tok[at, part].astype(f32), k_gain, cos, sin)
                k_inv[at, part] = inv
                for u in range(2):
                    g = lo // HEAD_CHANNELS + u
                    kr[g, at, :] = turned[:, u * HEAD_CHANNELS : (u + 1) * HEAD_CHANNELS]
                    begin = k_width + g * HEAD_CHANNELS
                    vv[g, at, :] = kv_tok[at, begin : begin + HEAD_CHANNELS]
        for r in range(q_rows):
            at = slice(r * GRID, (r + 1) * GRID)
            cos, sin = turn.angles_of(upper * q_rows + r)
            for lo in range(0, q_width, pair):
                part = slice(lo, lo + pair)
                inv, turned = turn.forward(q_tok[at, part].astype(f32), q_gain, cos, sin)
                q_inv[at, part] = inv
                grad = q_tok[at, q_width + lo : q_width + lo + pair]
                for u in range(2):
                    lanes = slice(u * HEAD_CHANNELS, (u + 1) * HEAD_CHANNELS)
                    qh[lo // HEAD_CHANNELS + u, at, :] = turned[:, lanes]
                    gh[lo // HEAD_CHANNELS + u, at, :] = grad[:, lanes]
        for g in range(groups):
            key_rot = kr[g]
            for h in range(g * per_group, (g + 1) * per_group):
                scores = dot(key_rot, qh[h], 1, 1)
                top = jnp.max(scores, axis=0, keepdims=True)
                expo = jnp.exp((scores - top) * score_scale)
                prob = expo * (1.0 / jnp.sum(expo, axis=0, keepdims=True))
                probs[h] = prob
                dv = dot(prob.astype(bf16), gh[h], 1, 0)
                value_acc = dv if h == g * per_group else value_acc + dv
            dv_sc[:, g * HEAD_CHANNELS : (g + 1) * HEAD_CHANNELS] = value_acc
        split_halves(dv_sc, upper, half, pv_own, pv_far)

    outs = kernel_call(
        body,
        [
            held((half, k_width), f32),
            held((half, k_width)),
            held((heads, tokens, half), f32),
            held((heads, half, HEAD_CHANNELS)),
            held((heads, half, HEAD_CHANNELS)),
            held((groups, tokens, HEAD_CHANNELS)),
            held((groups, tokens, HEAD_CHANNELS)),
            held((half, q_width), f32),
            held((tokens, k_width), f32),
            held((half, 2 * q_width)),
            held((tokens, 2 * k_width)),
        ],
        [pltpu.VMEM((tokens, k_width), f32)],
        (own, mate, far, far_mate, *gains, *tables),
        flops=4 * heads * half * tokens * HEAD_CHANNELS,
        limit=20 * MIB,
    )
    return outs[0], outs[1], outs[2:]


def attention_keys(state, gains, tables):
    probs, _, _, kr, _, q_inv, k_inv, _, _ = state
    heads, tokens, half = probs.shape
    rows = half // 2
    groups = kr.shape[0]
    per_group = heads // groups
    q_width, k_width = q_inv.shape[1], k_inv.shape[1]
    pair = 2 * HEAD_CHANNELS

    def body(*refs):
        probs, qh, gh, kr, vv, q_inv, k_inv, q_tok, kv_tok, qg_ref, kg_ref = refs[:11]
        dq_own, dq_mate, pk_own, pk_far, dq_sc, dk_sc, dq_out, p_sc = refs[15:]
        me = lax.axis_index("sp")
        bit = me % 2
        upper = me // 2
        turn = Rotation(*refs[11:15])
        q_gain = jnp.concatenate([qg_ref[...], qg_ref[...]], axis=1)
        k_gain = jnp.concatenate([kg_ref[...], kg_ref[...]], axis=1)
        q_rows = half // GRID
        for g in range(groups):
            key_rot = kr[g]
            value_in = vv[g]
            for h in range(g * per_group, (g + 1) * per_group):
                prob = probs[h]
                prob_grad = dot(value_in, gh[h], 1, 1)
                row_dot = jnp.sum(prob * prob_grad, axis=0, keepdims=True)
                score_grad = (prob * (prob_grad - row_dot)).astype(bf16)
                dk = dot(score_grad, qh[h], 1, 0)
                dq_t = dot(key_rot, score_grad, 0, 0)
                dq_sc[:, h * HEAD_CHANNELS : (h + 1) * HEAD_CHANNELS] = dq_t.T * score_scale
                key_acc = dk if h == g * per_group else key_acc + dk
            dk_sc[:, g * HEAD_CHANNELS : (g + 1) * HEAD_CHANNELS] = key_acc * score_scale
        for r in range(tokens // GRID):
            at = slice(r * GRID, (r + 1) * GRID)
            cos, sin = turn.angles_of(r)
            for lo in range(0, k_width, pair):
                part = slice(lo, lo + pair)
                value = kv_tok[at, part].astype(f32)
                p_sc[at, part] = turn.backward(
                    value, k_inv[at, part], dk_sc[at, part], k_gain, cos, sin
                )
        split_halves(p_sc, upper, half, pk_own, pk_far)
        for r in range(q_rows):
            at = slice(r * GRID, (r + 1) * GRID)
            cos, sin = turn.angles_of(upper * q_rows + r)
            for lo in range(0, q_width, pair):
                part = slice(lo, lo + pair)
                value = q_tok[at, part].astype(f32)
                result = turn.backward(value, q_inv[at, part], dq_sc[at, part], q_gain, cos, sin)
                dq_out[at, part] = result.astype(bf16)
        dq_own[...] = dq_out[pl.ds(pl.multiple_of(bit * rows, rows), rows), :]
        dq_mate[...] = dq_out[pl.ds(pl.multiple_of((1 - bit) * rows, rows), rows), :]

    return kernel_call(
        body,
        [held((rows, q_width))] * 2 + [held((half, k_width), f32), held((half, k_width))],
        [
            pltpu.VMEM((half, q_width), f32),
            pltpu.VMEM((tokens, k_width), f32),
            pltpu.VMEM((half, q_width), bf16),
            pltpu.VMEM((tokens, k_width), f32),
        ],
        (*state, *gains, *tables),
        flops=6 * heads * half * tokens * HEAD_CHANNELS,
        limit=20 * MIB,
    )


def weight_partials(turned, turned_mate, p_own, p_far, extra, dp_count):
    feats, rows = turned.shape
    half, cols = p_own.shape
    share = feats // dp_count
    chips = dp_count // 2

    def body(x_ref, xm_ref, po_ref, pf_ref, *rest):
        mine_out, mate_out, own_out, send_out, p_sc = rest[len(extra) :]
        bit = lax.axis_index("sp") % 2
        mine = lax.axis_index("dp")
        p_sc[...] = (po_ref[...] + pf_ref[...].astype(f32)).astype(bf16)
        p_mine = p_sc[pl.ds(pl.multiple_of(bit * rows, rows), rows), :]
        p_mate = p_sc[pl.ds(pl.multiple_of((1 - bit) * rows, rows), rows), :]
        mine_out[...] = p_mine
        mate_out[:, :cols] = p_mate
        lo = cols
        for ref in rest[: len(extra)]:
            mate_out[:, lo : lo + ref.shape[1]] = ref[...]
            lo += ref.shape[1]
        p_all = jnp.concatenate([p_mine, p_mate], axis=0)
        for out, flip in ((send_out, 1), (own_out, 0)):
            for m in range(chips):
                start = pl.multiple_of((mine ^ (2 * m + flip)) * share, share)
                at = pl.ds(start, share)
                x_all = jnp.concatenate([x_ref[at, :], xm_ref[at, :]], axis=1)
                out[m] = dot(x_all, p_all, 1, 0).astype(bf16)

    return kernel_call(
        body,
        [held((rows, cols)), held((rows, cols + sum(value.shape[1] for value in extra)))]
        + [held((chips, share, cols))] * 2,
        [pltpu.VMEM((half, cols), bf16)],
        (turned, turned_mate, p_own, p_far, *extra),
        flops=2 * feats * half * cols,
    )


def sum_cores(own, received):
    chips, share, cols = own.shape

    def body(own_ref, got_ref, first, *rest):
        first[...] = own_ref[0].astype(f32) + got_ref[0].astype(f32)
        for m, out in enumerate(rest, 1):
            out[...] = (own_ref[m].astype(f32) + got_ref[m].astype(f32)).astype(bf16)

    return kernel_call(
        body, [held((share, cols), f32)] + [held((share, cols))] * (chips - 1), [], (own, received)
    )


def sum_chips(first, received):
    def body(*refs):
        total = refs[0][...]
        for ref in refs[1:-1]:
            total = total + ref[...].astype(f32)
        refs[-1][...] = total.astype(bf16)

    return kernel_call(body, [held(first.shape)], [], (first, *received))[0]


def join_weight_grad(own, mate, far, far_mate):
    rows, cols = own.shape

    def body(own_ref, mate_ref, far_ref, far_mate_ref, out, scratch, sems):
        even = lax.axis_index("sp") % 2 == 0
        copies = []
        for i in range(2):
            at = slice(i * rows // 2, (i + 1) * rows // 2)
            here = own_ref[at, :].astype(f32) + far_ref[at, :].astype(f32)
            there = mate_ref[at, :].astype(f32) + far_mate_ref[at, :].astype(f32)
            scratch[at, :cols] = jnp.where(even, here, there)
            scratch[at, cols:] = jnp.where(even, there, here)
            copies.append(pltpu.make_async_copy(scratch.at[at, :], out.at[at, :], sems.at[i]))
            copies[-1].start()
        for copy in copies:
            copy.wait()

    return pl.pallas_call(
        body,
        out_shape=shape_of((rows, 2 * cols), f32),
        in_specs=[pl.BlockSpec(memory_space=pltpu.VMEM)] * 4,
        out_specs=pl.BlockSpec(memory_space=pltpu.HBM),
        scratch_shapes=[pltpu.VMEM((rows, 2 * cols), f32), pltpu.SemaphoreType.DMA((2,))],
        compiler_params=pltpu.CompilerParams(vmem_limit_bytes=4 * MIB),
    )(*[in_vmem(piece) for piece in (own, mate, far, far_mate)])


def token_outputs(k_mine, v_mine, from_mate, weight_pieces, dq_own):
    rows, cols = k_mine.shape
    q_half = dq_own.shape[1]
    dp_count = len(weight_pieces)
    w_rows = weight_pieces[0].shape[0]

    def body(k_ref, v_ref, mate_ref, dq_ref, *rest):
        w_refs = rest[:dp_count]
        x_out, q_out, p_buf, out_buf, q_buf = rest[dp_count:]
        bit = lax.axis_index("sp") % 2
        mine = lax.axis_index("dp")
        p_buf[bit] = jnp.concatenate([k_ref[...], v_ref[...]], axis=1)
        p_buf[1 - bit] = mate_ref[:, : 2 * cols]
        q_buf[bit] = dq_ref[...]
        q_buf[1 - bit] = mate_ref[:, 2 * cols :]
        for d in range(2):
            q_out[:, d * q_half : (d + 1) * q_half] = q_buf[d]
        left = jnp.concatenate([p_buf[0], p_buf[1]], axis=1)
        for m in range(dp_count):
            out_buf[mine ^ m] = dot(left, w_refs[m][...], 1, 1).astype(bf16)
        for j in range(dp_count):
            x_out[:, j * w_rows : (j + 1) * w_rows] = out_buf[j]

    return kernel_call(
        body,
        [shape_of((rows, dp_count * w_rows)), shape_of((rows, 2 * q_half))],
        [
            pltpu.VMEM((2, rows, 2 * cols), bf16),
            pltpu.VMEM((dp_count, rows, w_rows), bf16),
            pltpu.VMEM((2, rows, q_half), bf16),
        ],
        (k_mine, v_mine, from_mate, dq_own, *weight_pieces),
        flops=8 * rows * dp_count * w_rows * cols,
    )


def fast_device(
    inputs, queries, keys, values, out_grad, query_gain, key_gain, key_matrix, value_matrix
):
    return fast_body(
        inputs[0],
        queries[0],
        keys[0],
        values[0],
        out_grad[0],
        query_gain,
        key_gain,
        key_matrix,
        value_matrix,
    )


def fast_body(
    inputs, queries, keys, values, out_grad, query_gain, key_gain, key_matrix, value_matrix
):
    dp_count = lax.axis_size("dp")
    chips = dp_count // 2
    mate, far, far_mate = pack_heads(queries, keys, values, out_grad)
    mate = swap_with(mate, "sp", 1)
    far = swap_with(far, "sp", 2)
    far_mate = swap_with(far_mate, "sp", 3)
    tables = [jnp.asarray(table) for table in angle_tables(4 * inputs.shape[0])]
    own, joined_weight, *small = pack_own(
        queries,
        keys,
        values,
        out_grad,
        key_matrix,
        value_matrix,
        [query_gain[None], key_gain[None], *tables],
    )
    gains, tables = small[:2], small[2:]
    weight_pieces = [joined_weight] + [
        swap_with(joined_weight, "dp", m) for m in range(1, dp_count)
    ]
    mate_inputs = swap_with(inputs, "sp", 1)
    v_own, v_far, state = attention_values(own, mate, far, far_mate, gains, tables)
    v_far = swap_with(v_far, "sp", 2)
    dq_own, dq_mate, k_own, k_far = attention_keys(state, gains, tables)
    k_far = swap_with(k_far, "sp", 2)
    turned = turn_inputs(inputs)
    turned_mate = turn_inputs(mate_inputs)

    def weight_grad(p_own, p_far, extra):
        mine, there, blocks, sent = weight_partials(
            turned, turned_mate, p_own, p_far, extra, dp_count
        )
        first, *rest = sum_cores(blocks, swap_with(sent, "dp", 1))
        received = [swap_with(rest[m - 1], "dp", 2 * m) for m in range(1, chips)]
        total = sum_chips(first, received)
        others = [swap_with(total, "sp", k) for k in range(1, 4)]
        return mine, there, join_weight_grad(total, *others)

    v_mine, v_there, value_weight = weight_grad(v_own, v_far, ())
    k_mine, there, key_weight = weight_grad(k_own, k_far, (v_there, dq_mate))
    from_mate = swap_with(there, "sp", 1)
    input_grad, query_grad = token_outputs(k_mine, v_mine, from_mate, weight_pieces, dq_own)
    return input_grad[None], query_grad[None], key_weight, value_weight


def solution(mesh):
    sp_count, dp_count = mesh.shape["sp"], mesh.shape["dp"]
    fast = sp_count == 4 and dp_count & (dp_count - 1) == 0
    return jax.shard_map(
        fast_device if fast else generic_device,
        mesh=mesh,
        in_specs=(
            P("dp", "sp", None),
            P("dp", "sp", None),
            P("dp", "sp", None),
            P("dp", "sp", None),
            P("dp", "sp", None),
            P(),
            P(),
            P("dp", None),
            P("dp", None),
        ),
        out_specs=(P("dp", "sp", None), P("dp", "sp", None), P("dp", None), P("dp", None)),
        check_vma=False,
    )
```
